32 devices in a mesh: ep: 8 (over z, y), tp: 4 (over x, core).
Axes of the slice: x: 2, y: 2, z: 4, core: 2. Of those that a mesh axis runs over, the one named last changes fastest.
Arguments:
- tokens: bfloat16 [512, 1024], P('ep', 'tp'), may hold values from -6 to 6
- conv_state: bfloat16 [512, 3, 512], P('ep', None, 'tp'), may hold values from -6 to 6
- lru_state: float32 [512, 512], P('ep', 'tp'), may hold values from -6 to 6
- mix_gain: bfloat16 [1024], replicated, may hold values from 0.099609375 to 1.8984375
- ffn_gain: bfloat16 [1024], replicated, may hold values from 0.099609375 to 1.8984375
- w_branch: bfloat16 [1024, 512], P(None, 'tp'), may hold values from -0.1875 to 0.1875
- w_gate: bfloat16 [1024, 512], P(None, 'tp'), may hold values from -0.1875 to 0.1875
- conv_taps: bfloat16 [4, 512], P(None, 'tp'), may hold values from -3 to 3
- w_recur: bfloat16 [8, 64, 64], P('tp'), may hold values from -0.75 to 0.75
- w_inject: bfloat16 [8, 64, 64], P('tp'), may hold values from -0.75 to 0.75
- lru_lambda: float32 [512], P('tp'), may hold values from 2 to 7
- w_out: bfloat16 [512, 1024], P('tp'), may hold values from -0.25 to 0.25
- expert_gate: bfloat16 [8, 1024, 2560], P('ep', None, 'tp'), may hold values from -0.1875 to 0.1875
- expert_up: bfloat16 [8, 1024, 2560], P('ep', None, 'tp'), may hold values from -0.1875 to 0.1875
- expert_down: bfloat16 [8, 2560, 1024], P('ep', 'tp'), may hold values from -0.125 to 0.125
- route_ids: int32 [512, 2], P('ep'), may hold values from 0 to 7, all different within a row; in each aligned block of 64 rows (0 to 63, 64 to 127, ...) at most 32 rows name the same one
- route_weight: float32 [512, 2], P('ep'), may hold values from 0.2 to 1
Outputs:
- mixed: bfloat16 [512, 1024], P('ep', 'tp')
- state_out: float32 [512, 512], P('ep', 'tp')
The draws below stay inside these ranges and needn't reach their ends.
Inputs may be any that keep to these rules, and one draw needn't show every extreme that they name: `route_ids`: each row names 2 different experts. Among the 64 rows of one device no expert is named more than 32 times, and in every draw some expert is named exactly 32 times by them.
All inputs are finite; a program needn't handle non-finite values.
Results may differ from the reference program's by a relative error of at most 0.015.
Values may be sent and summed in bfloat16 or wider, within the bound.
No kernel may reach another device: no remote copies, remote signals or barrier semaphores. Data moves between devices by JAX's collectives and lax.ppermute only.
A program may use at most 64 MiB of HBM per device.

```python
import math
import jax
import jax.numpy as jnp
import numpy as np
from jax import lax

D = 1024
HEADS = 8
HEAD_W = 64
W_A = 512
CONV = 4
FF = 2560
SEQS = 64
TOP = 2
EXPERTS = 8
CAP = 32
SEQ_ALL = 512
N_TP = 4


def block_levels(stream_key, dims, shards, smallest, largest):
    loudness = 1.0
    for axis_at, shards_of in shards:
        heights = jax.random.uniform(jax.random.fold_in(jax.random.fold_in(stream_key, 6), axis_at), (shards_of,), jnp.float32, smallest / len(shards), largest / len(shards))
        loudness = loudness * jnp.repeat(jnp.exp(heights), dims[axis_at] // shards_of).reshape((-1,) + (1,) * (len(dims) - 1 - axis_at))
    return loudness


def routed_block(rng, own, number, rows, number_of, top, reach, skew):
    ranking = jax.random.permutation(rng, number_of)
    packed, usual = shares(number_of, rows * top, reach, skew, True), shares(number_of, rows * top, reach, skew, False)
    places = jnp.arange(number_of)

    def named(tallies, rotation):
        used = int((tallies > 0).sum())
        fixed = max(1, used // 4)
        moved = fixed + (places - fixed + rotation * (used - fixed)) % max(1, number_of - fixed)
        return jnp.zeros((number_of,), jnp.int32).at[ranking[jnp.where(places < fixed, places, moved)]].set(jnp.asarray(tallies, jnp.int32))

    tallies = jnp.where(number % 4 == 0, named(packed, number // 4), named(usual, number - number // 4 - 1))
    mixed = jax.random.permutation(jax.random.fold_in(own, 3), number_of)
    donor, sink = mixed[0:number_of // 2 * 2:2], mixed[1:number_of // 2 * 2:2]
    slack = jnp.minimum(tallies[donor] - 1, reach - tallies[sink]) // 2
    slack = jnp.where((donor == ranking[0]) | (sink == ranking[0]) | (tallies[sink] == 0), 0, jnp.maximum(slack, 0))
    moved = jax.random.randint(jax.random.fold_in(own, 4), (number_of // 2,), 0, 1 << 20) % (slack + 1)
    tallies = tallies.at[donor].add(-moved).at[sink].add(moved)
    items = jnp.searchsorted(jnp.cumsum(tallies), jnp.arange(rows * top), side="right").astype(jnp.int32)
    table = items.reshape(top, rows).T
    table = table[jax.random.permutation(jax.random.fold_in(own, 1), rows)]
    rotation = jax.random.randint(jax.random.fold_in(own, 2), (rows, 1), 0, top)
    return jnp.take_along_axis(table, (jnp.arange(top)[None, :] + rotation) % top, axis=1)


def shares(count, total, reach, skew, full):
    loads = [(1 << 20) // math.isqrt(grade ** skew) + 1 for grade in range(1, count + 1)]
    largest = reach if full else min(reach, max(-(-total // count), total * loads[0] // sum(loads)))
    least = 1 if total - largest >= count - 1 else 0
    given, surplus = [largest] + [least] * (count - 1), total - largest - least * (count - 1)
    while surplus > 0:
        candidates = [i for i in range(1, count) if given[i] < largest] or [i for i in range(1, count) if given[i] < reach]
        whole, remaining = sum([loads[i] for i in candidates]), surplus
        for i in candidates:
            extra = min(reach - given[i], max(1, remaining * loads[i] // whole), surplus)
            given[i] = given[i] + extra
            surplus = surplus - extra
    return np.array(given)


def gaussian(stream_key, dims, spread, limit, pieces=(), kind=jnp.bfloat16):
    factor_of = block_levels(stream_key, dims, pieces, -0.22, 0.18) if pieces else 1.0
    result = jax.random.normal(stream_key, dims, jnp.float32) * spread * factor_of
    return jnp.minimum(jnp.maximum(result, -limit), limit).astype(kind)


def setup_inputs(seed: int = 0) -> dict:
    splits = jax.random.split(jax.random.key(seed), 18)
    tokens = gaussian(splits[0], (SEQ_ALL, D), 1.0, 6.0, ((0, 8), (1, 4)))
    conv_state = gaussian(splits[1], (SEQ_ALL, CONV - 1, W_A), 1.0, 6.0, ((0, 8), (2, 4)))
    lru_state = gaussian(splits[2], (SEQ_ALL, W_A), 1.0, 6.0, ((0, 8), (1, 4)), jnp.float32)
    mix_gain = jnp.clip(1.0 + 0.18 * jax.random.normal(splits[3], (D,), jnp.float32), 0.099609375, 1.8984375).astype(jnp.bfloat16)
    ffn_gain = jnp.clip(1.0 + 0.18 * jax.random.normal(splits[4], (D,), jnp.float32), 0.099609375, 1.8984375).astype(jnp.bfloat16)
    w_branch = gaussian(splits[5], (D, W_A), D ** -0.5, 0.1875, ((1, 4),))
    w_gate = gaussian(splits[6], (D, W_A), D ** -0.5, 0.1875, ((1, 4),))
    conv_taps = gaussian(splits[7], (CONV, W_A), 0.5, 3.0, ((1, 4),))
    w_recur = gaussian(splits[8], (HEADS, HEAD_W, HEAD_W), HEAD_W ** -0.5, 0.75, ((0, 4),))
    w_inject = gaussian(splits[9], (HEADS, HEAD_W, HEAD_W), HEAD_W ** -0.5, 0.75, ((0, 4),))
    lru_lambda = jnp.clip(2.0 + 5.0 * jax.random.uniform(splits[10], (W_A,), jnp.float32) ** block_levels(splits[10], (W_A,), ((0, 4),), -0.2, 0.2), 2.0, 7.0)
    w_out = gaussian(splits[11], (W_A, D), W_A ** -0.5, 0.25, ((0, 4),))
    expert_gate = gaussian(splits[12], (EXPERTS, D, FF), D ** -0.5, 0.1875, ((0, 8), (2, 4)))
    expert_up = gaussian(splits[13], (EXPERTS, D, FF), D ** -0.5, 0.1875, ((0, 8), (2, 4)))
    expert_down = gaussian(splits[14], (EXPERTS, FF, D), FF ** -0.5, 0.125, ((0, 8), (1, 4)))
    route_ids_keys = jax.random.split(jax.random.fold_in(splits[15], 1), SEQ_ALL // SEQS)
    route_ids_turns = jax.random.permutation(jax.random.fold_in(splits[15], 3), SEQ_ALL // SEQS)
    route_ids = jax.vmap(lambda own, number: routed_block(jax.random.fold_in(splits[15], 2), own, number, SEQS, EXPERTS, TOP, CAP, 2))(route_ids_keys, route_ids_turns).reshape((SEQ_ALL, TOP))
    route_weight = jnp.clip(0.2 + 0.8 * jax.random.uniform(splits[16], (SEQ_ALL, TOP), jnp.float32) ** block_levels(splits[16], (SEQ_ALL, TOP), ((0, 8),), -0.2, 0.2), 0.2, 1.0)
    return {"tokens": tokens, "conv_state": conv_state, "lru_state": lru_state, "mix_gain": mix_gain, "ffn_gain": ffn_gain, "w_branch": w_branch, "w_gate": w_gate, "conv_taps": conv_taps, "w_recur": w_recur, "w_inject": w_inject, "lru_lambda": lru_lambda, "w_out": w_out, "expert_gate": expert_gate, "expert_up": expert_up, "expert_down": expert_down, "route_ids": route_ids, "route_weight": route_weight}


EPS = 1e-06
LRU_SCALE = 8.0

def rms_rows(rows, gain):
    values = rows.astype(jnp.float32)
    scaled = values * lax.rsqrt(lax.optimization_barrier(jnp.mean(values * values, axis=-1, keepdims=True)) + EPS)
    return (scaled * gain.astype(jnp.float32)).astype(jnp.bfloat16)

def split_sum(left, right, groups):
    count = left.shape[0]
    width = left.shape[1] // groups
    parts = jnp.einsum('ngk,gkm->ngm', left.reshape(count, groups, width).astype(jnp.float32), right.reshape(groups, width, right.shape[1]).astype(jnp.float32))
    rounded = lax.optimization_barrier(parts.astype(jnp.bfloat16)).astype(jnp.float32)
    return lax.optimization_barrier(jnp.sum(rounded, axis=1)).astype(jnp.bfloat16)

def reference(tokens, conv_state, lru_state, mix_gain, ffn_gain, w_branch, w_gate, conv_taps, w_recur, w_inject, lru_lambda, w_out, expert_gate, expert_up, expert_down, route_ids, route_weight):
    count = tokens.shape[0]
    normed = rms_rows(tokens, mix_gain)
    branch = jnp.dot(normed, w_branch, preferred_element_type=jnp.float32).astype(jnp.bfloat16)
    gate_in = jnp.dot(normed, w_gate, preferred_element_type=jnp.float32).astype(jnp.bfloat16)
    window = jnp.concatenate([conv_state, branch[:, None, :]], axis=1).astype(jnp.float32)
    conv_out = lax.optimization_barrier(jnp.sum(window * conv_taps.astype(jnp.float32)[None], axis=1))
    conv_heads = lax.optimization_barrier(conv_out.astype(jnp.bfloat16)).astype(jnp.float32).reshape(count, HEADS, HEAD_W)
    recur = jax.nn.sigmoid(jnp.einsum('nhi,hij->nhj', conv_heads, w_recur.astype(jnp.float32)).reshape(count, HEADS * HEAD_W))
    inject = jax.nn.sigmoid(jnp.einsum('nhi,hij->nhj', conv_heads, w_inject.astype(jnp.float32)).reshape(count, HEADS * HEAD_W))
    log_decay = -LRU_SCALE * recur * jax.nn.softplus(-lru_lambda)
    state_out = jnp.exp(log_decay) * lru_state + jnp.sqrt(-jnp.expm1(2.0 * log_decay)) * inject * conv_out
    lru_out = (state_out * jax.nn.gelu(gate_in.astype(jnp.float32))).astype(jnp.bfloat16)
    mix_out = split_sum(lru_out, w_out, N_TP)
    resid = (tokens.astype(jnp.float32) + mix_out.astype(jnp.float32)).astype(jnp.bfloat16)
    normed2 = rms_rows(resid, ffn_gain)
    groups = count // SEQS
    flat = route_ids.reshape(groups, SEQS * TOP).astype(jnp.int32)
    onehot = (flat[:, :, None] == jnp.arange(EXPERTS, dtype=jnp.int32)[None, None, :]).astype(jnp.int32)
    before = jnp.cumsum(onehot, axis=1) - onehot
    slot = lax.optimization_barrier(jnp.sum(before * onehot, axis=2)).astype(jnp.int32)
    where = (jnp.arange(groups, dtype=jnp.int32)[:, None] * CAP + slot).reshape(-1).astype(jnp.int32)
    token_of = (jnp.arange(groups, dtype=jnp.int32)[:, None] * SEQS + jnp.arange(SEQS * TOP, dtype=jnp.int32)[None, :] // TOP).reshape(-1).astype(jnp.int32)
    expert_of = flat.reshape(-1)
    table = jnp.full((EXPERTS, groups * CAP), count, jnp.int32).at[expert_of, where].set(token_of)
    padded = jnp.concatenate([normed2, jnp.zeros((1, D), jnp.bfloat16)], axis=0)

    def one_expert(args):
        rows_idx, e_gate, e_up, e_down = args
        rows = padded[rows_idx].astype(jnp.float32)
        first = jnp.dot(rows, e_gate.astype(jnp.float32))
        second = jnp.dot(rows, e_up.astype(jnp.float32))
        hidden = (jax.nn.silu(first) * second).astype(jnp.bfloat16)
        return split_sum(hidden, e_down, N_TP)
    outputs = lax.map(one_expert, (table, expert_gate, expert_up, expert_down))
    picked = outputs[expert_of, where].reshape(count, TOP, D).astype(jnp.float32)
    moe = lax.optimization_barrier(jnp.sum(picked * route_weight[:, :, None], axis=1))
    mixed = (resid.astype(jnp.float32) + moe).astype(jnp.bfloat16)
    return (mixed, state_out)
```

```python
import jax
import jax.numpy as jnp
import numpy as np
from jax import lax
from jax.sharding import Mesh, PartitionSpec as P

EPS = 1e-06
LRU_SCALE = 8.0
SWAP = ((0, 1), (1, 0))


def rms_rows(rows, gain):
    values = rows.astype(jnp.float32)
    scaled = values * lax.rsqrt(jnp.mean(values * values, axis=-1, keepdims=True) + EPS)
    return (scaled * gain.astype(jnp.float32)).astype(jnp.bfloat16)


def body(
    tokens,
    conv_state,
    lru_state,
    mix_gain,
    ffn_gain,
    w_branch,
    w_gate,
    conv_taps,
    w_recur,
    w_inject,
    lru_lambda,
    w_out,
    expert_gate,
    expert_up,
    expert_down,
    route_ids,
    route_weight,
):
    seqs, quarter = tokens.shape
    n_ep = lax.axis_size("ep")
    tp = ("xa", "xb")
    na, nb = lax.axis_size("xa"), lax.axis_size("xb")
    n_tp = na * nb
    me = lax.axis_index(tp)
    others = [
        lax.ppermute(tokens, tp, [(i, i ^ k) for i in range(n_tp)]) for k in range(1, n_tp)
    ]
    pieces = jnp.stack([tokens] + others)
    whole = jnp.concatenate(
        [lax.dynamic_index_in_dim(pieces, me ^ t, 0, keepdims=False) for t in range(n_tp)], axis=1
    )
    normed = rms_rows(whole, mix_gain)
    branch = jnp.dot(normed, w_branch, preferred_element_type=jnp.float32).astype(jnp.bfloat16)
    gate_in = jnp.dot(normed, w_gate, preferred_element_type=jnp.float32).astype(jnp.bfloat16)
    window = jnp.concatenate([conv_state, branch[:, None, :]], axis=1).astype(jnp.float32)
    conv_out = jnp.sum(window * conv_taps.astype(jnp.float32)[None], axis=1)
    heads_here = w_recur.shape[0]
    head_width = w_recur.shape[1]
    conv_heads = conv_out.astype(jnp.bfloat16).reshape(seqs, heads_here, head_width)
    recur = jax.nn.sigmoid(
        jnp.einsum("nhi,hij->nhj", conv_heads, w_recur, preferred_element_type=jnp.float32).reshape(
            seqs, -1
        )
    )
    inject = jax.nn.sigmoid(
        jnp.einsum(
            "nhi,hij->nhj", conv_heads, w_inject, preferred_element_type=jnp.float32
        ).reshape(seqs, -1)
    )
    log_decay = -LRU_SCALE * recur * jax.nn.softplus(-lru_lambda)
    state_out = (
        jnp.exp(log_decay) * lru_state + jnp.sqrt(-jnp.expm1(2.0 * log_decay)) * inject * conv_out
    )
    lru_out = (state_out * jax.nn.gelu(gate_in.astype(jnp.float32))).astype(jnp.bfloat16)
    partial_value = jnp.dot(lru_out, w_out, preferred_element_type=jnp.float32).astype(jnp.bfloat16)
    split = partial_value.reshape(seqs, n_tp, quarter)
    mix_out = lax.dynamic_index_in_dim(split, me, 1, keepdims=False).astype(jnp.float32)
    for k in range(1, n_tp):
        out = lax.dynamic_index_in_dim(split, me ^ k, 1, keepdims=False)
        mix_out = mix_out + lax.ppermute(
            out, tp, [(i, i ^ k) for i in range(n_tp)]
        ).astype(jnp.float32)
    resid = (tokens.astype(jnp.float32) + mix_out.astype(jnp.bfloat16).astype(jnp.float32)).astype(
        jnp.bfloat16
    )
    top = route_ids.shape[1]
    local = expert_gate.shape[0]
    experts = n_ep * local
    capacity = max(2, 2 * seqs * top // experts)
    slots = experts * capacity
    flat = route_ids.reshape(-1)
    onehot = (flat[:, None] == jnp.arange(experts, dtype=jnp.int32)[None, :]).astype(jnp.int32)
    before = jnp.cumsum(onehot, axis=0) - onehot
    slot = jnp.sum(before * onehot, axis=1)
    slot_id = flat * capacity + slot
    hits = (slot_id.reshape(seqs, top)[:, :, None] == jnp.arange(slots, dtype=jnp.int32)).astype(
        jnp.bfloat16
    )
    dispatch = jnp.sum(hits, axis=1)
    buffer = lax.dot_general(
        dispatch, resid, (((0,), (0,)), ((), ())), preferred_element_type=jnp.float32
    ).astype(jnp.bfloat16)
    sent = jnp.broadcast_to(buffer[None], (na, slots, quarter)).reshape(na * slots, quarter)
    mine = lax.all_to_all(sent, ("xa", "ep"), split_axis=0, concat_axis=0, tiled=True)
    theirs = lax.ppermute(mine, "xb", SWAP)
    b = lax.axis_index("xb")
    first_b = jnp.where(b == 0, mine, theirs).reshape(na, slots, quarter)
    second_b = jnp.where(b == 0, theirs, mine).reshape(na, slots, quarter)
    rows = jnp.stack([first_b, second_b], axis=1).transpose(2, 0, 1, 3).reshape(slots, -1)
    rows = rms_rows(rows, ffn_gain)
    first = jnp.dot(rows, expert_gate[0], preferred_element_type=jnp.float32)
    second = jnp.dot(rows, expert_up[0], preferred_element_type=jnp.float32)
    hidden = (jax.nn.silu(first) * second).astype(jnp.bfloat16)
    term = jnp.dot(hidden, expert_down[0], preferred_element_type=jnp.float32).astype(jnp.bfloat16)
    term = term.reshape(slots, na, nb, quarter).transpose(2, 1, 0, 3).reshape(nb, na * slots, quarter)
    keep = lax.dynamic_index_in_dim(term, b, 0, keepdims=False)
    give = lax.dynamic_index_in_dim(term, 1 - b, 0, keepdims=False)
    pair = (
        keep.astype(jnp.float32) + lax.ppermute(give, "xb", SWAP).astype(jnp.float32)
    ).astype(jnp.bfloat16)
    back = lax.all_to_all(pair, ("xa", "ep"), split_axis=0, concat_axis=0, tiled=True)
    back = back.reshape(na, slots, quarter)
    moe = jnp.zeros((seqs, quarter), jnp.float32)
    for k in range(top):
        picked = sum(
            jnp.dot(hits[:, k], back[a], preferred_element_type=jnp.float32) for a in range(na)
        )
        moe = moe + picked * route_weight[:, k, None]
    mixed = (resid.astype(jnp.float32) + moe).astype(jnp.bfloat16)
    return (mixed, state_out)


def solution(mesh):
    n_ep, n_tp = mesh.shape["ep"], mesh.shape["tp"]
    finer = Mesh(np.asarray(mesh.devices).reshape(n_ep, n_tp // 2, 2), ("ep", "xa", "xb"))
    tp = ("xa", "xb")
    placed = (
        P("ep", tp),
        P("ep", None, tp),
        P("ep", tp),
        P(),
        P(),
        P(None, tp),
        P(None, tp),
        P(None, tp),
        P(tp, None, None),
        P(tp, None, None),
        P(tp),
        P(tp, None),
        P("ep", None, tp),
        P("ep", None, tp),
        P("ep", tp, None),
        P("ep", None),
        P("ep", None),
    )
    return jax.shard_map(
        body, mesh=finer, in_specs=placed, out_specs=(P("ep", tp), P("ep", tp)), check_vma=False
    )
```

```python
import jax
import jax.numpy as jnp
import numpy as np
from jax import lax
from jax.experimental import pallas as pl
from jax.experimental.pallas import tpu as pltpu
from jax.sharding import Mesh, PartitionSpec as P

EPS = 1e-06
LRU_SCALE = 8.0
SWAP = ((0, 1), (1, 0))
F32, BF16 = jnp.float32, jnp.bfloat16


def call(kernel, outs, *args, scratch=(), flops=0, final=(), limit=4 << 20, far=0):
    away = tuple(pltpu.with_memory_space_constraint(a, pltpu.HBM) for a in args[:far])
    near = tuple(pltpu.with_memory_space_constraint(a, pltpu.VMEM) for a in args[far:])
    return pl.pallas_call(
        kernel,
        out_shape=[
            jax.ShapeDtypeStruct(s, d) if i in final else pltpu.VMEM(s, d)
            for i, (s, d) in enumerate(outs)
        ],
        in_specs=[pl.BlockSpec(memory_space=pltpu.HBM)] * far
        + [pl.BlockSpec(memory_space=pltpu.VMEM)] * len(near),
        out_specs=[pl.BlockSpec(memory_space=pltpu.VMEM)] * len(outs),
        scratch_shapes=list(scratch),
        compiler_params=pltpu.CompilerParams(vmem_limit_bytes=limit),
        cost_estimate=pl.CostEstimate(flops=flops, bytes_accessed=0, transcendentals=0),
    )(*away, *near)


def dot(a, b):
    return jnp.dot(a, b, preferred_element_type=F32)


def tp_index():
    return lax.axis_index("xa") * lax.axis_size("xb") + lax.axis_index("xb")


def span(i, size):
    return pl.ds(pl.multiple_of(i * size, size), size)


def prepare(experts, capacity):
    def kernel(*refs):
        small, large, refs = refs[:9], refs[9:14], refs[14:]
        place, wcol, older, last_tap, gates, rate, mix_row, ffn_row = refs[:8]
        placed, held, sem, large_sem = refs[8:13], refs[13:22], refs[22], refs[23]
        copies = [pltpu.make_async_copy(a, b, sem.at[i]) for i, (a, b) in enumerate(zip(small, held))]
        more = [
            pltpu.make_async_copy(a, b, large_sem.at[i]) for i, (a, b) in enumerate(zip(large, placed))
        ]
        for c in copies + more:
            c.start()
        for c in copies:
            c.wait()
        ids, weight, conv, taps, wr, wi, lam, mix_gain, ffn_gain = held
        top, seqs = ids.shape
        earlier = (
            lax.broadcasted_iota(jnp.int32, (seqs, seqs), 0)
            < lax.broadcasted_iota(jnp.int32, (seqs, seqs), 1)
        ).astype(BF16)
        same = lax.broadcasted_iota(jnp.int32, (seqs, seqs), 0) == lax.broadcasted_iota(
            jnp.int32, (seqs, seqs), 1
        )
        number = lax.broadcasted_iota(jnp.int32, (experts, seqs), 0)
        base = jnp.zeros((experts, 1), F32)
        for k in range(top):
            row = ids[k : k + 1, :]
            named = (number == row).astype(F32)
            before = dot(named.astype(BF16), earlier) + base
            slot = jnp.sum(before * named, axis=0, keepdims=True)
            place[k : k + 1, :] = row * capacity + slot.astype(jnp.int32)
            base = base + jnp.sum(named, axis=1, keepdims=True)
            column = jnp.sum(jnp.where(same, weight[k : k + 1, :], 0.0), axis=1, keepdims=True)
            wcol[k] = jnp.broadcast_to(column, wcol.shape[1:])
        total = conv[0].astype(F32) * taps[0:1, :].astype(F32)
        for j in range(1, conv.shape[0]):
            total = total + conv[j].astype(F32) * taps[j : j + 1, :].astype(F32)
        older[...] = total
        last_tap[...] = taps[conv.shape[0] :, :].astype(F32)
        heads, width = wr.shape[0], wr.shape[1]
        gates[...] = jnp.zeros_like(gates)
        for h in range(heads):
            at = slice(h * width, (h + 1) * width)
            gates[at, at] = wr[h]
            gates[at, heads * width + h * width : heads * width + (h + 1) * width] = wi[h]
        rate[...] = -LRU_SCALE * jnp.log1p(jnp.exp(-lam[...])).reshape(rate.shape)
        mix_row[...] = mix_gain[...].astype(F32).reshape(mix_row.shape)
        ffn_row[...] = ffn_gain[...].astype(F32).reshape(ffn_row.shape)
        for c in more:
            c.wait()

    return kernel


def load(*refs):
    *refs, done, sem = refs
    n = len(refs) // 2
    done[...] = jnp.zeros_like(done)
    copies = [pltpu.make_async_copy(refs[i], refs[n + 1 + i], sem.at[i]) for i in range(n)]
    for c in copies:
        c.start()
    for c in copies:
        c.wait()


def mixer(t0, t1, t2, t3, mix_row, w_branch, w_gate, older, last_tap, gates, rate, state, w_out, state_out, p0, p1, p2, p3):
    me = tp_index()
    quarter = t0.shape[1]
    pieces = [t[...].astype(F32) for t in (t0, t1, t2, t3)]
    squares = sum(jnp.sum(p * p, axis=1, keepdims=True) for p in pieces)
    scale = lax.rsqrt(squares / (len(pieces) * quarter) + EPS)
    branch = gate_in = 0.0
    for k, p in enumerate(pieces):
        at = span(me ^ k, quarter)
        normed = (p * scale * mix_row[:, at]).astype(BF16)
        branch = branch + dot(normed, w_branch[at, :])
        gate_in = gate_in + dot(normed, w_gate[at, :])
    branch = branch.astype(BF16).astype(F32)
    gate_in = gate_in.astype(BF16).astype(F32)
    conv_out = older[...] + branch * last_tap[...]
    both = dot(conv_out.astype(BF16), gates[...])
    channels = conv_out.shape[1]
    recur = jax.nn.sigmoid(both[:, :channels])
    inject = jax.nn.sigmoid(both[:, channels:])
    log_decay = recur * rate[...]
    y = -2.0 * log_decay
    series = y * (1.0 - y * (1 / 2) * (1.0 - y * (1 / 3) * (1.0 - y * (1 / 4) * (1.0 - y * (1 / 5)))))
    left = jnp.where(y < 0.1, series, 1.0 - jnp.exp(-y))
    out = jnp.exp(log_decay) * state[...] + jnp.sqrt(left) * inject * conv_out
    state_out[...] = out
    lru_out = (out * jax.nn.gelu(gate_in)).astype(BF16)
    for k, p in enumerate((p0, p1, p2, p3)):
        p[...] = dot(lru_out, w_out[:, span(me ^ k, quarter)]).astype(BF16)


def hits_of(place, k, slots):
    return lax.broadcasted_iota(jnp.int32, (slots, place.shape[1]), 0) == place[k : k + 1, :]


def send_rows(tokens, p0, p1, p2, p3, place, loaded, resid, sent):
    mix_out = sum(p[...].astype(F32) for p in (p0, p1, p2, p3)).astype(BF16).astype(F32)
    rows = (tokens[...].astype(F32) + mix_out).astype(BF16)
    resid[...] = rows
    copies = lax.axis_size("xa")
    slots = sent.shape[0] // copies
    named = sum(hits_of(place, k, slots).astype(F32) for k in range(place.shape[0])).astype(BF16)
    buffer = dot(named, rows).astype(BF16)
    for a in range(copies):
        sent[a * slots : (a + 1) * slots, :] = buffer


def experts_of(mine, theirs, ffn_row, w_gate, w_up, w_down, keep, give, rows):
    b = lax.axis_index("xb")
    na, nb = lax.axis_size("xa"), lax.axis_size("xb")
    slots, quarter = mine.shape[0] // na, mine.shape[1]
    squares = 0.0
    for a in range(na):
        for part in (mine, theirs):
            v = part[a * slots : (a + 1) * slots, :].astype(F32)
            squares = squares + jnp.sum(v * v, axis=1, keepdims=True)
    scale = lax.rsqrt(squares / rows.shape[1] + EPS)
    for a in range(na):
        for part, c in ((mine, b), (theirs, 1 - b)):
            at = span(a * nb + c, quarter)
            v = part[a * slots : (a + 1) * slots, :].astype(F32)
            rows[:, at] = (v * scale * ffn_row[:, at]).astype(BF16)
    first = dot(rows[...], w_gate[0])
    second = dot(rows[...], w_up[0])
    hidden = (jax.nn.silu(first) * second).astype(BF16)
    for a in range(na):
        for part, c in ((give, 1 - b), (keep, b)):
            at = span(a * nb + c, quarter)
            part[a * slots : (a + 1) * slots, :] = dot(hidden, w_down[0, :, at]).astype(BF16)


def add_pair(keep, other, out):
    out[...] = (keep[...].astype(F32) + other[...].astype(F32)).astype(BF16)


def combine(resid, back, place, wcol, mixed):
    slots = back.shape[0] // lax.axis_size("xa")
    width = wcol.shape[2]
    total = [resid[:, i : i + width].astype(F32) for i in range(0, resid.shape[1], width)]
    for k in range(place.shape[0]):
        named = hits_of(place, k, slots).astype(F32).astype(BF16)
        picked = sum(
            lax.dot_general(
                named, back[a : a + slots, :], (((0,), (0,)), ((), ())), preferred_element_type=F32
            )
            for a in range(0, back.shape[0], slots)
        )
        for i in range(len(total)):
            total[i] = total[i] + picked[:, i * width : (i + 1) * width] * wcol[k]
    for i, v in enumerate(total):
        mixed[:, i * width : (i + 1) * width] = v.astype(BF16)


def body(
    tokens,
    conv_state,
    lru_state,
    mix_gain,
    ffn_gain,
    w_branch,
    w_gate,
    conv_taps,
    w_recur,
    w_inject,
    lru_lambda,
    w_out,
    expert_gate,
    expert_up,
    expert_down,
    route_ids,
    route_weight,
):
    seqs, quarter = tokens.shape
    top = route_ids.shape[1]
    channels = lru_state.shape[1]
    tp = ("xa", "xb")
    na = lax.axis_size("xa")
    n_tp = na * lax.axis_size("xb")
    features = n_tp * quarter
    experts = lax.axis_size("ep") * expert_gate.shape[0]
    capacity = max(2, 2 * seqs * top // experts)
    slots = experts * capacity

    def swapped(x, k):
        return lax.ppermute(x, tp, [(i, i ^ k) for i in range(n_tp)])

    others = [swapped(tokens, k) for k in range(1, n_tp)]
    small = (
        route_ids.T,
        route_weight.T,
        conv_state.transpose(1, 0, 2),
        conv_taps,
        w_recur,
        w_inject,
        lru_lambda,
        mix_gain,
        ffn_gain,
    )
    large = (tokens, lru_state, w_branch, w_gate, w_out)
    place, wcol, older, last_tap, gates, rate, mix_row, ffn_row, here, state, w_b, w_g, w_o = call(
        prepare(experts, capacity),
        [
            ((top, seqs), jnp.int32),
            ((top, seqs, 128), F32),
            ((seqs, channels), F32),
            ((1, channels), F32),
            ((channels, 2 * channels), BF16),
            ((1, channels), F32),
            ((1, features), F32),
            ((1, features), F32),
        ]
        + [(a.shape, a.dtype) for a in large],
        *small,
        *large,
        far=len(small) + len(large),
        scratch=[pltpu.VMEM(a.shape, a.dtype) for a in small]
        + [pltpu.SemaphoreType.DMA((len(small),)), pltpu.SemaphoreType.DMA((len(large),))],
        flops=10**6,
    )
    state_out, *parts = call(
        mixer,
        [((seqs, channels), F32)] + [((seqs, quarter), BF16)] * n_tp,
        here,
        *others,
        mix_row,
        w_b,
        w_g,
        older,
        last_tap,
        gates,
        rate,
        state,
        w_o,
        flops=10**8,
        final=(0,),
    )
    weights = (expert_gate, expert_up, expert_down)
    w_eg, w_eu, w_ed, loaded = call(
        load,
        [(a.shape, a.dtype) for a in weights] + [((8, 128), F32)],
        *weights,
        parts[0],
        far=len(weights),
        scratch=[pltpu.SemaphoreType.DMA((len(weights),))],
        flops=10**6,
    )
    got = [parts[0]] + [swapped(parts[k], k) for k in range(1, n_tp)]
    resid, sent = call(
        send_rows,
        [((seqs, quarter), BF16), ((na * slots, quarter), BF16)],
        here,
        *got,
        place,
        loaded,
        flops=10**7,
    )
    mine = lax.all_to_all(sent, ("xa", "ep"), split_axis=0, concat_axis=0, tiled=True)
    theirs = lax.ppermute(mine, "xb", SWAP)
    keep, give = call(
        experts_of,
        [((na * slots, quarter), BF16)] * 2,
        mine,
        theirs,
        ffn_row,
        w_eg,
        w_eu,
        w_ed,
        scratch=[pltpu.VMEM((slots, features), BF16)],
        flops=10**9,
        limit=10 << 20,
    )
    (pair,) = call(add_pair, [((na * slots, quarter), BF16)], keep, lax.ppermute(give, "xb", SWAP))
    back = lax.all_to_all(pair, ("xa", "ep"), split_axis=0, concat_axis=0, tiled=True)
    (mixed,) = call(combine, [((seqs, quarter), BF16)], resid, back, place, wcol, final=(0,))
    return (mixed, state_out)


def solution(mesh):
    n_ep, n_tp = mesh.shape["ep"], mesh.shape["tp"]
    finer = Mesh(np.asarray(mesh.devices).reshape(n_ep, n_tp // 2, 2), ("ep", "xa", "xb"))
    tp = ("xa", "xb")
    placed = (
        P("ep", tp),
        P("ep", None, tp),
        P("ep", tp),
        P(),
        P(),
        P(None, tp),
        P(None, tp),
        P(None, tp),
        P(tp, None, None),
        P(tp, None, None),
        P(tp),
        P(tp, None),
        P("ep", None, tp),
        P("ep", None, tp),
        P("ep", tp, None),
        P("ep", None),
        P("ep", None),
    )
    return jax.shard_map(
        body, mesh=finer, in_specs=placed, out_specs=(P("ep", tp), P("ep", tp)), check_vma=False
    )
```

```python
import jax
import jax.numpy as jnp
import numpy as np
from jax import lax
from jax.experimental import pallas as pl
from jax.experimental.pallas import tpu as pltpu
from jax.sharding import Mesh, PartitionSpec as P

EPS = 1e-06
LRU_SCALE = 8.0
SWAP = ((0, 1), (1, 0))
F32, BF16 = jnp.float32, jnp.bfloat16


def call(kernel, outs, *args, scratch=(), flops=0, final=(), limit=4 << 20, far=0):
    away = tuple(pltpu.with_memory_space_constraint(a, pltpu.HBM) for a in args[:far])
    near = tuple(pltpu.with_memory_space_constraint(a, pltpu.VMEM) for a in args[far:])
    return pl.pallas_call(
        kernel,
        out_shape=[
            jax.ShapeDtypeStruct(s, d) if i in final else pltpu.VMEM(s, d)
            for i, (s, d) in enumerate(outs)
        ],
        in_specs=[pl.BlockSpec(memory_space=pltpu.HBM)] * far
        + [pl.BlockSpec(memory_space=pltpu.VMEM)] * len(near),
        out_specs=[pl.BlockSpec(memory_space=pltpu.VMEM)] * len(outs),
        scratch_shapes=list(scratch),
        compiler_params=pltpu.CompilerParams(vmem_limit_bytes=limit),
        cost_estimate=pl.CostEstimate(flops=flops, bytes_accessed=0, transcendentals=0),
    )(*away, *near)


def dot(a, b):
    return jnp.dot(a, b, preferred_element_type=F32)


def tp_index():
    return lax.axis_index("xa") * lax.axis_size("xb") + lax.axis_index("xb")


def span(i, size):
    return pl.ds(pl.multiple_of(i * size, size), size)


def prepare(experts, capacity):
    def prepare_kernel(*refs):
        small, large, refs = refs[:9], refs[9:15], refs[15:]
        place, wcol, older, last_tap, gates, rate, mix_row, ffn_row = refs[:8]
        placed, held, sem, large_sem = refs[8:14], refs[14:23], refs[23], refs[24]
        copies = [pltpu.make_async_copy(a, b, sem.at[i]) for i, (a, b) in enumerate(zip(small, held))]
        more = [
            pltpu.make_async_copy(a, b, large_sem.at[i]) for i, (a, b) in enumerate(zip(large, placed))
        ]
        for c in copies + more:
            c.start()
        for c in copies:
            c.wait()
        ids, weight, conv, taps, wr, wi, lam, mix_gain, ffn_gain = held
        top, seqs = ids.shape
        earlier = (
            lax.broadcasted_iota(jnp.int32, (seqs, seqs), 0)
            < lax.broadcasted_iota(jnp.int32, (seqs, seqs), 1)
        ).astype(BF16)
        same = lax.broadcasted_iota(jnp.int32, (seqs, seqs), 0) == lax.broadcasted_iota(
            jnp.int32, (seqs, seqs), 1
        )
        number = lax.broadcasted_iota(jnp.int32, (experts, seqs), 0)
        base = jnp.zeros((experts, 1), F32)
        for k in range(top):
            row = ids[k : k + 1, :]
            named = (number == row).astype(F32)
            before = dot(named.astype(BF16), earlier) + base
            slot = jnp.sum(before * named, axis=0, keepdims=True)
            place[k : k + 1, :] = row * capacity + slot.astype(jnp.int32)
            base = base + jnp.sum(named, axis=1, keepdims=True)
            column = jnp.sum(jnp.where(same, weight[k : k + 1, :], 0.0), axis=1, keepdims=True)
            wcol[k] = jnp.broadcast_to(column, wcol.shape[1:])
        total = conv[0].astype(F32) * taps[0:1, :].astype(F32)
        for j in range(1, conv.shape[0]):
            total = total + conv[j].astype(F32) * taps[j : j + 1, :].astype(F32)
        older[...] = total
        last_tap[...] = taps[conv.shape[0] :, :].astype(F32)
        heads, width = wr.shape[0], wr.shape[1]
        gates[...] = jnp.zeros_like(gates)
        for h in range(heads):
            at = slice(h * width, (h + 1) * width)
            gates[at, at] = wr[h]
            gates[at, heads * width + h * width : heads * width + (h + 1) * width] = wi[h]
        rate[...] = -LRU_SCALE * jnp.log1p(jnp.exp(-lam[...])).reshape(rate.shape)
        mix_row[...] = mix_gain[...].astype(F32).reshape(mix_row.shape)
        ffn_row[...] = ffn_gain[...].astype(F32).reshape(ffn_row.shape)
        for c in more:
            c.wait()

    return prepare_kernel


def load(*refs):
    *refs, done, sem = refs
    n = len(refs) // 2
    done[...] = jnp.zeros_like(done)
    copies = [pltpu.make_async_copy(refs[i], refs[n + 1 + i], sem.at[i]) for i in range(n)]
    for c in copies:
        c.start()
    for c in copies:
        c.wait()


def mixer(t0, t1, t2, t3, mix_row, w_branch, w_gate, older, last_tap, gates, rate, state, w_out, state_out, p0, p1, p2, p3):
    me = tp_index()
    quarter = t0.shape[1]
    pieces = [t[...].astype(F32) for t in (t0, t1, t2, t3)]
    squares = sum(jnp.sum(p * p, axis=1, keepdims=True) for p in pieces)
    scale = lax.rsqrt(squares / (len(pieces) * quarter) + EPS)
    branch = gate_in = 0.0
    for k, p in enumerate(pieces):
        at = span(me ^ k, quarter)
        normed = (p * scale * mix_row[:, at]).astype(BF16)
        branch = branch + dot(normed, w_branch[at, :])
        gate_in = gate_in + dot(normed, w_gate[at, :])
    branch = branch.astype(BF16).astype(F32)
    gate_in = gate_in.astype(BF16).astype(F32)
    conv_out = older[...] + branch * last_tap[...]
    both = dot(conv_out.astype(BF16), gates[...])
    channels = conv_out.shape[1]
    recur = jax.nn.sigmoid(both[:, :channels])
    inject = jax.nn.sigmoid(both[:, channels:])
    log_decay = recur * rate[...]
    y = -2.0 * log_decay
    series = y * (1.0 - y * (1 / 2) * (1.0 - y * (1 / 3) * (1.0 - y * (1 / 4) * (1.0 - y * (1 / 5)))))
    left = jnp.where(y < 0.1, series, 1.0 - jnp.exp(-y))
    out = jnp.exp(log_decay) * state[...] + jnp.sqrt(left) * inject * conv_out
    state_out[...] = out
    lru_out = (out * jax.nn.gelu(gate_in)).astype(BF16)
    for k, p in enumerate((p0, p1, p2, p3)):
        p[...] = dot(lru_out, w_out[:, span(me ^ k, quarter)]).astype(BF16)


def hits_of(place, k, slots):
    return lax.broadcasted_iota(jnp.int32, (slots, place.shape[1]), 0) == place[k : k + 1, :]


def send_rows(tokens, p0, p1, p2, p3, place, loaded, resid, sent):
    mix_out = sum(p[...].astype(F32) for p in (p0, p1, p2, p3)).astype(BF16).astype(F32)
    rows = (tokens[...].astype(F32) + mix_out).astype(BF16)
    resid[...] = rows
    copies = lax.axis_size("xa")
    slots = sent.shape[0] // copies
    named = sum(hits_of(place, k, slots).astype(F32) for k in range(place.shape[0])).astype(BF16)
    buffer = dot(named, rows).astype(BF16)
    for a in range(copies):
        sent[a * slots : (a + 1) * slots, :] = buffer


def own_half(mine, ffn_row, w_gate, w_up, first, second, squares):
    b = lax.axis_index("xb")
    na, nb = lax.axis_size("xa"), lax.axis_size("xb")
    slots, quarter = mine.shape[0] // na, mine.shape[1]
    f = s = total = 0.0
    for a in range(na):
        at = span(a * nb + b, quarter)
        v = mine[a * slots : (a + 1) * slots, :].astype(F32)
        total = total + jnp.sum(v * v, axis=1, keepdims=True)
        u = (v * ffn_row[:, at]).astype(BF16)
        f = f + dot(u, w_gate[0, at, :])
        s = s + dot(u, w_up[0, at, :])
    first[...] = f
    second[...] = s
    squares[...] = jnp.broadcast_to(total, squares.shape)


def other_half(theirs, ffn_row, w_gate, w_up, w_down, first, second, squares, hidden, give):
    b = 1 - lax.axis_index("xb")
    na, nb = lax.axis_size("xa"), lax.axis_size("xb")
    slots, quarter = theirs.shape[0] // na, theirs.shape[1]
    f, s, total = first[...], second[...], squares[:, :1]
    for a in range(na):
        at = span(a * nb + b, quarter)
        v = theirs[a * slots : (a + 1) * slots, :].astype(F32)
        total = total + jnp.sum(v * v, axis=1, keepdims=True)
        u = (v * ffn_row[:, at]).astype(BF16)
        f = f + dot(u, w_gate[0, at, :])
        s = s + dot(u, w_up[0, at, :])
    scale = lax.rsqrt(total / (na * nb * quarter) + EPS)
    h = (jax.nn.silu(f * scale) * (s * scale)).astype(BF16)
    hidden[...] = h
    for a in range(na):
        give[a * slots : (a + 1) * slots, :] = dot(h, w_down[0, :, span(a * nb + b, quarter)]).astype(BF16)


def kept_half(hidden, w_down, keep):
    b = lax.axis_index("xb")
    na, nb = lax.axis_size("xa"), lax.axis_size("xb")
    slots, quarter = hidden.shape[0], keep.shape[1]
    for a in range(na):
        at = span(a * nb + b, quarter)
        keep[a * slots : (a + 1) * slots, :] = dot(hidden[...], w_down[0, :, at]).astype(BF16)


def add_pair(keep, other, out):
    out[...] = (keep[...].astype(F32) + other[...].astype(F32)).astype(BF16)


def combine(resid, back, place, wcol, mixed):
    slots = back.shape[0] // lax.axis_size("xa")
    width = wcol.shape[2]
    total = [resid[:, i : i + width].astype(F32) for i in range(0, resid.shape[1], width)]
    for k in range(place.shape[0]):
        named = hits_of(place, k, slots).astype(F32).astype(BF16)
        picked = sum(
            lax.dot_general(
                named, back[a : a + slots, :], (((0,), (0,)), ((), ())), preferred_element_type=F32
            )
            for a in range(0, back.shape[0], slots)
        )
        for i in range(len(total)):
            total[i] = total[i] + picked[:, i * width : (i + 1) * width] * wcol[k]
    for i, v in enumerate(total):
        mixed[:, i * width : (i + 1) * width] = v.astype(BF16)


def step(
    tokens,
    conv_state,
    lru_state,
    mix_gain,
    ffn_gain,
    w_branch,
    w_gate,
    conv_taps,
    w_recur,
    w_inject,
    lru_lambda,
    w_out,
    expert_gate,
    expert_up,
    expert_down,
    route_ids,
    route_weight,
):
    seqs, quarter = tokens.shape
    top = route_ids.shape[1]
    channels = lru_state.shape[1]
    tp = ("xa", "xb")
    na = lax.axis_size("xa")
    n_tp = na * lax.axis_size("xb")
    features = n_tp * quarter
    experts = lax.axis_size("ep") * expert_gate.shape[0]
    capacity = max(2, 2 * seqs * top // experts)
    slots = experts * capacity

    def swapped(x, k):
        return lax.ppermute(x, tp, [(i, i ^ k) for i in range(n_tp)])

    others = [swapped(tokens, k) for k in range(1, n_tp)]
    small = (
        route_ids.T,
        route_weight.T,
        conv_state.transpose(1, 0, 2),
        conv_taps,
        w_recur,
        w_inject,
        lru_lambda,
        mix_gain,
        ffn_gain,
    )
    large = (tokens, lru_state, w_branch, w_gate, w_out, expert_down)
    place, wcol, older, last_tap, gates, rate, mix_row, ffn_row, here, state, w_b, w_g, w_o, w_ed = call(
        prepare(experts, capacity),
        [
            ((top, seqs), jnp.int32),
            ((top, seqs, 128), F32),
            ((seqs, channels), F32),
            ((1, channels), F32),
            ((channels, 2 * channels), BF16),
            ((1, channels), F32),
            ((1, features), F32),
            ((1, features), F32),
        ]
        + [(a.shape, a.dtype) for a in large],
        *small,
        *large,
        far=len(small) + len(large),
        scratch=[pltpu.VMEM(a.shape, a.dtype) for a in small]
        + [pltpu.SemaphoreType.DMA((len(small),)), pltpu.SemaphoreType.DMA((len(large),))],
        flops=10**6,
    )
    state_out, *parts = call(
        mixer,
        [((seqs, channels), F32)] + [((seqs, quarter), BF16)] * n_tp,
        here,
        *others,
        mix_row,
        w_b,
        w_g,
        older,
        last_tap,
        gates,
        rate,
        state,
        w_o,
        flops=10**8,
        final=(0,),
    )
    weights = (expert_gate, expert_up)
    w_eg, w_eu, loaded = call(
        load,
        [(a.shape, a.dtype) for a in weights] + [((8, 128), F32)],
        *weights,
        parts[0],
        far=len(weights),
        scratch=[pltpu.SemaphoreType.DMA((len(weights),))],
        flops=10**6,
    )
    got = [parts[0]] + [swapped(parts[k], k) for k in range(1, n_tp)]
    resid, sent = call(
        send_rows,
        [((seqs, quarter), BF16), ((na * slots, quarter), BF16)],
        here,
        *got,
        place,
        loaded,
        flops=10**7,
    )
    mine = lax.all_to_all(sent, ("xa", "ep"), split_axis=0, concat_axis=0, tiled=True)
    theirs = lax.ppermute(mine, "xb", SWAP)
    ff = expert_gate.shape[2]
    first, second, squares = call(
        own_half,
        [((slots, ff), F32), ((slots, ff), F32), ((slots, 128), F32)],
        mine,
        ffn_row,
        w_eg,
        w_eu,
        flops=10**8,
        limit=8 << 20,
    )
    hidden, give = call(
        other_half,
        [((slots, ff), BF16), ((na * slots, quarter), BF16)],
        theirs,
        ffn_row,
        w_eg,
        w_eu,
        w_ed,
        first,
        second,
        squares,
        flops=10**8,
        limit=8 << 20,
    )
    other = lax.ppermute(give, "xb", SWAP)
    (keep,) = call(kept_half, [((na * slots, quarter), BF16)], hidden, w_ed, flops=10**8)
    (pair,) = call(add_pair, [((na * slots, quarter), BF16)], keep, other)
    back = lax.all_to_all(pair, ("xa", "ep"), split_axis=0, concat_axis=0, tiled=True)
    (mixed,) = call(combine, [((seqs, quarter), BF16)], resid, back, place, wcol, final=(0,))
    return (mixed, state_out)


def solution(mesh):
    n_ep, n_tp = mesh.shape["ep"], mesh.shape["tp"]
    finer = Mesh(np.asarray(mesh.devices).reshape(n_ep, n_tp // 2, 2), ("ep", "xa", "xb"))
    tp = ("xa", "xb")
    placed = (
        P("ep", tp),
        P("ep", None, tp),
        P("ep", tp),
        P(),
        P(),
        P(None, tp),
        P(None, tp),
        P(None, tp),
        P(tp, None, None),
        P(tp, None, None),
        P(tp),
        P(tp, None),
        P("ep", None, tp),
        P("ep", None, tp),
        P("ep", tp, None),
        P("ep", None),
        P("ep", None),
    )
    return jax.shard_map(step, mesh=finer, in_specs=placed, out_specs=(P("ep", tp), P("ep", tp)), check_vma=False)
```

```python
import jax
import jax.numpy as jnp
import numpy as np
from jax import lax
from jax.experimental import pallas as pl
from jax.experimental.pallas import tpu as pltpu
from jax.sharding import Mesh, PartitionSpec as P

EPS = 1e-06
LRU_SCALE = 8.0
SWAP = ((0, 1), (1, 0))
F32, BF16 = jnp.float32, jnp.bfloat16


def call(kernel, outs, *args, scratch=(), flops=0, final=(), limit=4 << 20, far=0):
    away = tuple(pltpu.with_memory_space_constraint(a, pltpu.HBM) for a in args[:far])
    near = tuple(pltpu.with_memory_space_constraint(a, pltpu.VMEM) for a in args[far:])
    return pl.pallas_call(
        kernel,
        out_shape=[
            jax.ShapeDtypeStruct(s, d) if i in final else pltpu.VMEM(s, d)
            for i, (s, d) in enumerate(outs)
        ],
        in_specs=[pl.BlockSpec(memory_space=pltpu.HBM)] * far
        + [pl.BlockSpec(memory_space=pltpu.VMEM)] * len(near),
        out_specs=[pl.BlockSpec(memory_space=pltpu.VMEM)] * len(outs),
        scratch_shapes=list(scratch),
        compiler_params=pltpu.CompilerParams(vmem_limit_bytes=limit),
        cost_estimate=pl.CostEstimate(flops=flops, bytes_accessed=0, transcendentals=0),
    )(*away, *near)


def dot(a, b):
    return jnp.dot(a, b, preferred_element_type=F32)


def tp_index():
    return lax.axis_index("xa") * lax.axis_size("xb") + lax.axis_index("xb")


def span(i, size):
    return pl.ds(pl.multiple_of(i * size, size), size)


def prepare(experts, half):
    def prepare_kernel(*refs):
        small, large, refs = refs[:9], refs[9:15], refs[15:]
        named, hits, wcol, older, last_tap, gates, rate, mix_row, ffn_row = refs[:9]
        placed, held, sem, large_sem = refs[9:15], refs[15:24], refs[24], refs[25]
        copies = [pltpu.make_async_copy(a, b, sem.at[i]) for i, (a, b) in enumerate(zip(small, held))]
        more = [
            pltpu.make_async_copy(a, b, large_sem.at[i]) for i, (a, b) in enumerate(zip(large, placed))
        ]
        for c in copies + more:
            c.start()
        for c in copies:
            c.wait()
        ids, weight, conv, taps, wr, wi, lam, mix_gain, ffn_gain = held
        top, seqs = ids.shape
        earlier = (
            lax.broadcasted_iota(jnp.int32, (seqs, seqs), 0)
            < lax.broadcasted_iota(jnp.int32, (seqs, seqs), 1)
        ).astype(BF16)
        same = lax.broadcasted_iota(jnp.int32, (seqs, seqs), 0) == lax.broadcasted_iota(
            jnp.int32, (seqs, seqs), 1
        )
        number = lax.broadcasted_iota(jnp.int32, (experts, seqs), 0)
        base = jnp.zeros((experts, 1), F32)
        slots = named.shape[0]
        down = lax.broadcasted_iota(jnp.int32, (slots, seqs), 0).astype(F32)
        across = lax.broadcasted_iota(jnp.int32, (seqs, slots), 1).astype(F32)
        sent = jnp.zeros((slots, seqs), F32)
        for k in range(top):
            row = ids[k : k + 1, :]
            mine = (number == row).astype(F32)
            before = dot(mine.astype(BF16), earlier) + base
            slot = jnp.sum(before * mine, axis=0, keepdims=True)
            base = base + jnp.sum(mine, axis=1, keepdims=True)
            part = jnp.floor((slot + 0.5) * (1 / half))
            place = part * (experts * half) + row.astype(F32) * half + (slot - part * half)
            sent = sent + (down == place).astype(F32)
            column = jnp.sum(jnp.where(same, place, 0.0), axis=1, keepdims=True)
            hits[k * seqs : (k + 1) * seqs, :] = (across == column).astype(F32).astype(BF16)
            column = jnp.sum(jnp.where(same, weight[k : k + 1, :], 0.0), axis=1, keepdims=True)
            wcol[k] = jnp.broadcast_to(column, wcol.shape[1:])
        named[...] = sent.astype(BF16)
        total = conv[0].astype(F32) * taps[0:1, :].astype(F32)
        for j in range(1, conv.shape[0]):
            total = total + conv[j].astype(F32) * taps[j : j + 1, :].astype(F32)
        older[...] = total
        last_tap[...] = taps[conv.shape[0] :, :].astype(F32)
        heads, width = wr.shape[0], wr.shape[1]
        gates[...] = jnp.zeros_like(gates)
        for h in range(heads):
            at = slice(h * width, (h + 1) * width)
            gates[at, at] = wr[h]
            gates[at, heads * width + h * width : heads * width + (h + 1) * width] = wi[h]
        rate[...] = -LRU_SCALE * jnp.log1p(jnp.exp(-lam[...])).reshape(rate.shape)
        mix_row[...] = mix_gain[...].astype(F32).reshape(mix_row.shape)
        ffn_row[...] = ffn_gain[...].astype(F32).reshape(ffn_row.shape)
        for c in more:
            c.wait()

    return prepare_kernel


def load(*refs):
    *refs, done, sem = refs
    n = len(refs) // 2
    done[...] = jnp.zeros_like(done)
    copies = [pltpu.make_async_copy(refs[i], refs[n + 1 + i], sem.at[i]) for i in range(n)]
    for c in copies:
        c.start()
    for c in copies:
        c.wait()


def mixer(t0, t1, t2, t3, mix_row, w_branch, w_gate, older, last_tap, gates, rate, state, w_out, state_out, p0, p1, p2, p3):
    me = tp_index()
    quarter = t0.shape[1]
    pieces = [t[...].astype(F32) for t in (t0, t1, t2, t3)]
    squares = sum(jnp.sum(p * p, axis=1, keepdims=True) for p in pieces)
    scale = lax.rsqrt(squares / (len(pieces) * quarter) + EPS)
    branch = gate_in = 0.0
    for k, p in enumerate(pieces):
        at = span(me ^ k, quarter)
        normed = (p * scale * mix_row[:, at]).astype(BF16)
        branch = branch + dot(normed, w_branch[at, :])
        gate_in = gate_in + dot(normed, w_gate[at, :])
    branch = branch.astype(BF16).astype(F32)
    gate_in = gate_in.astype(BF16).astype(F32)
    conv_out = older[...] + branch * last_tap[...]
    both = dot(conv_out.astype(BF16), gates[...])
    channels = conv_out.shape[1]
    recur = jax.nn.sigmoid(both[:, :channels])
    inject = jax.nn.sigmoid(both[:, channels:])
    log_decay = recur * rate[...]
    y = -2.0 * log_decay
    series = y * (1.0 - y * (1 / 2) * (1.0 - y * (1 / 3) * (1.0 - y * (1 / 4) * (1.0 - y * (1 / 5)))))
    left = jnp.where(y < 0.1, series, 1.0 - jnp.exp(-y))
    out = jnp.exp(log_decay) * state[...] + jnp.sqrt(left) * inject * conv_out
    state_out[...] = out
    lru_out = (out * jax.nn.gelu(gate_in)).astype(BF16)
    for k, p in enumerate((p0, p1, p2, p3)):
        p[...] = dot(lru_out, w_out[:, span(me ^ k, quarter)]).astype(BF16)


def send_rows(tokens, p0, p1, p2, p3, named, loaded, resid, sent):
    mix_out = sum(p[...].astype(F32) for p in (p0, p1, p2, p3)).astype(BF16).astype(F32)
    rows = (tokens[...].astype(F32) + mix_out).astype(BF16)
    resid[...] = rows
    slots = named.shape[0]
    buffer = dot(named[...], rows).astype(BF16)
    for a in range(0, sent.shape[0], slots):
        sent[a : a + slots, :] = buffer


def experts_of(got, ffn_row, g0, u0, d0, g1, u1, d1, out, rows):
    count, quarter = rows.shape[0], got.shape[1]
    squares = 0.0
    for a in range(0, got.shape[0], count):
        v = got[a : a + count, :].astype(F32)
        squares = squares + jnp.sum(v * v, axis=1, keepdims=True)
    scale = lax.rsqrt(squares / rows.shape[1] + EPS)
    for t in range(got.shape[0] // count):
        at = slice(t * quarter, (t + 1) * quarter)
        v = got[t * count : (t + 1) * count, :].astype(F32)
        rows[:, at] = (v * scale * ffn_row[:, at]).astype(BF16)
    term = 0.0
    for g, u, d in ((g0, u0, d0), (g1, u1, d1)):
        hidden = (jax.nn.silu(dot(rows[...], g[0])) * dot(rows[...], u[0])).astype(BF16)
        term = term + dot(hidden, d[0])
    for t in range(got.shape[0] // count):
        out[t * count : (t + 1) * count, :] = term[:, t * quarter : (t + 1) * quarter].astype(BF16)


def combine(resid, back, hits, wcol, mixed):
    top, seqs, width = wcol.shape
    slots = hits.shape[1]
    picked = sum(dot(hits[...], back[a : a + slots, :]) for a in range(0, back.shape[0], slots))
    for i in range(0, resid.shape[1], width):
        total = resid[:, i : i + width].astype(F32)
        for k in range(top):
            total = total + picked[k * seqs : (k + 1) * seqs, i : i + width] * wcol[k]
        mixed[:, i : i + width] = total.astype(BF16)


def step(
    tokens,
    conv_state,
    lru_state,
    mix_gain,
    ffn_gain,
    w_branch,
    w_gate,
    conv_taps,
    w_recur,
    w_inject,
    lru_lambda,
    w_out,
    expert_gate,
    expert_up,
    expert_down,
    route_ids,
    route_weight,
):
    seqs, quarter = tokens.shape
    top = route_ids.shape[1]
    channels = lru_state.shape[1]
    tp = ("xa", "xb")
    na = lax.axis_size("xa")
    n_tp = na * lax.axis_size("xb")
    features = n_tp * quarter
    experts = lax.axis_size("ep") * expert_gate.shape[0]
    nb = lax.axis_size("xb")
    capacity = max(2, 2 * seqs * top // experts)
    half = -(-capacity // nb)
    slots = nb * experts * half
    ring = ("xa", "xb", "ep")

    def swapped(x, k):
        return lax.ppermute(x, tp, [(i, i ^ k) for i in range(n_tp)])

    others = [swapped(tokens, k) for k in range(1, n_tp)]
    small = (
        route_ids.T,
        route_weight.T,
        conv_state.transpose(1, 0, 2),
        conv_taps,
        w_recur,
        w_inject,
        lru_lambda,
        mix_gain,
        ffn_gain,
    )
    large = (tokens, lru_state, w_branch, w_gate, w_out, expert_down)
    named, hits, wcol, older, last_tap, gates, rate, mix_row, ffn_row, *brought = call(
        prepare(experts, half),
        [
            ((slots, seqs), BF16),
            ((top * seqs, slots), BF16),
            ((top, seqs, 128), F32),
            ((seqs, channels), F32),
            ((1, channels), F32),
            ((channels, 2 * channels), BF16),
            ((1, channels), F32),
            ((1, features), F32),
            ((1, features), F32),
        ]
        + [(a.shape, a.dtype) for a in large],
        *small,
        *large,
        far=len(small) + len(large),
        scratch=[pltpu.VMEM(a.shape, a.dtype) for a in small]
        + [pltpu.SemaphoreType.DMA((len(small),)), pltpu.SemaphoreType.DMA((len(large),))],
        flops=10**6,
    )
    here, state, w_b, w_g, w_o, w_down = brought
    state_out, *parts = call(
        mixer,
        [((seqs, channels), F32)] + [((seqs, quarter), BF16)] * n_tp,
        here,
        *others,
        mix_row,
        w_b,
        w_g,
        older,
        last_tap,
        gates,
        rate,
        state,
        w_o,
        flops=10**8,
        final=(0,),
    )
    weights = (expert_up, expert_gate)
    w_up, w_in, loaded = call(
        load,
        [(a.shape, a.dtype) for a in weights] + [((8, 128), F32)],
        *weights,
        parts[0],
        far=len(weights),
        scratch=[pltpu.SemaphoreType.DMA((len(weights),))],
        flops=10**6,
    )
    got = [parts[0]] + [swapped(parts[k], k) for k in range(1, n_tp)]
    resid, sent = call(
        send_rows,
        [((seqs, quarter), BF16), ((na * slots, quarter), BF16)],
        here,
        *got,
        named,
        loaded,
        flops=10**7,
    )
    partners = []
    for w in (w_in, w_up, w_down):
        partners.append(lax.ppermute(w, "xb", SWAP))
    arrived = lax.all_to_all(sent, ring, split_axis=0, concat_axis=0, tiled=True)
    (term,) = call(
        experts_of,
        [((na * slots, quarter), BF16)],
        arrived,
        ffn_row,
        w_in,
        w_up,
        w_down,
        *partners,
        scratch=[pltpu.VMEM((slots // nb, features), BF16)],
        flops=10**9,
        limit=8 << 20,
    )
    back = lax.all_to_all(term, ring, split_axis=0, concat_axis=0, tiled=True)
    (mixed,) = call(combine, [((seqs, quarter), BF16)], resid, back, hits, wcol, final=(0,))
    return (mixed, state_out)


def solution(mesh):
    n_ep, n_tp = mesh.shape["ep"], mesh.shape["tp"]
    finer = Mesh(np.asarray(mesh.devices).reshape(n_ep, n_tp // 2, 2), ("ep", "xa", "xb"))
    tp = ("xa", "xb")
    placed = (
        P("ep", tp),
        P("ep", None, tp),
        P("ep", tp),
        P(),
        P(),
        P(None, tp),
        P(None, tp),
        P(None, tp),
        P(tp, None, None),
        P(tp, None, None),
        P(tp),
        P(tp, None),
        P("ep", None, tp),
        P("ep", None, tp),
        P("ep", tp, None),
        P("ep", None),
        P("ep", None),
    )
    return jax.shard_map(step, mesh=finer, in_specs=placed, out_specs=(P("ep", tp), P("ep", tp)), check_vma=False)
```

```python
import jax
import jax.numpy as jnp
import numpy as np
from jax import lax
from jax.experimental import pallas as pl
from jax.experimental.pallas import tpu as pltpu
from jax.sharding import Mesh, PartitionSpec as P

EPS = 1e-06
LRU_SCALE = 8.0
SWAP = ((0, 1), (1, 0))
F32, BF16 = jnp.float32, jnp.bfloat16


def call(kernel, outs, *args, scratch=(), flops=0, final=(), limit=4 << 20, far=0):
    away = tuple(pltpu.with_memory_space_constraint(a, pltpu.HBM) for a in args[:far])
    near = tuple(pltpu.with_memory_space_constraint(a, pltpu.VMEM) for a in args[far:])
    return pl.pallas_call(
        kernel,
        out_shape=[
            jax.ShapeDtypeStruct(s, d) if i in final else pltpu.VMEM(s, d)
            for i, (s, d) in enumerate(outs)
        ],
        in_specs=[pl.BlockSpec(memory_space=pltpu.HBM)] * far
        + [pl.BlockSpec(memory_space=pltpu.VMEM)] * len(near),
        out_specs=[pl.BlockSpec(memory_space=pltpu.VMEM)] * len(outs),
        scratch_shapes=list(scratch),
        compiler_params=pltpu.CompilerParams(vmem_limit_bytes=limit),
        cost_estimate=pl.CostEstimate(flops=flops, bytes_accessed=0, transcendentals=0),
    )(*away, *near)


def dot(a, b):
    return jnp.dot(a, b, preferred_element_type=F32)


def tp_index():
    return lax.axis_index("xa") * lax.axis_size("xb") + lax.axis_index("xb")


def span(i, size):
    return pl.ds(pl.multiple_of(i * size, size), size)


def pack(conv_h, taps_h, wr_h, wi_h, lam_h, state_h, tok_h, rows, tok, conv, taps, wr, wi, lam, sem):
    seqs, channels = state_h.shape
    held = (conv, taps, wr, wi, lam)
    targets = held + (rows.at[seqs : 2 * seqs, :], tok)
    sources = (conv_h, taps_h, wr_h, wi_h, lam_h, state_h, tok_h)
    copies = [
        pltpu.make_async_copy(h, v, sem.at[i]) for i, (h, v) in enumerate(zip(sources, targets))
    ]
    for c in copies:
        c.start()
    ends = 2 * seqs
    rows[ends:, :] = jnp.zeros((rows.shape[0] - ends, channels), F32)
    for c in copies[: len(held)]:
        c.wait()
    total = conv[0].astype(F32) * taps[0:1, :].astype(F32)
    for j in range(1, conv.shape[0]):
        total = total + conv[j].astype(F32) * taps[j : j + 1, :].astype(F32)
    rows[:seqs, :] = total
    rows[ends : ends + 1, :] = taps[conv.shape[0] :, :].astype(F32)
    rows[ends + 1 : ends + 2, :] = -LRU_SCALE * jnp.log1p(jnp.exp(-lam[...])).reshape(1, -1)
    heads, width = wr.shape[0], wr.shape[1]
    for i, w in enumerate((wr, wi)):
        base = ends + 8 + i * channels
        for h in range(heads):
            at = slice(h * width, (h + 1) * width)
            rows[base + h * width : base + (h + 1) * width, at] = w[h].astype(F32)
    for c in copies[len(held) :]:
        c.wait()
    base = ends + 8 + 2 * channels
    for i in range(tok.shape[1] // channels):
        at = slice(i * channels, (i + 1) * channels)
        rows[base + i * seqs : base + (i + 1) * seqs, :] = tok[:, at].astype(F32)


def prepare(mix_h, ffn_h, b_h, g_h, o_h, _, mix_row, ffn_row, b, g, o, mix_gain, ffn_gain, sem):
    pairs = ((mix_h, mix_gain), (ffn_h, ffn_gain), (b_h, b), (g_h, g), (o_h, o))
    copies = [pltpu.make_async_copy(h, v, sem.at[i]) for i, (h, v) in enumerate(pairs)]
    for c in copies:
        c.start()
    for c in copies[:2]:
        c.wait()
    mix_row[...] = mix_gain[...].astype(F32).reshape(mix_row.shape)
    ffn_row[...] = ffn_gain[...].astype(F32).reshape(ffn_row.shape)
    for c in copies[2:]:
        c.wait()


def pick(experts, half):
    def pick_kernel(ids_h, weight_h, _, named, hits, wcol, ids, weight, sem):
        copies = [
            pltpu.make_async_copy(h, v, sem.at[i])
            for i, (h, v) in enumerate(((ids_h, ids), (weight_h, weight)))
        ]
        for c in copies:
            c.start()
        top, seqs = ids.shape
        slots = named.shape[0]
        one, other = (lax.broadcasted_iota(jnp.int32, (seqs, seqs), i) for i in range(2))
        earlier = (one < other).astype(BF16)
        number = lax.broadcasted_iota(jnp.int32, (experts, seqs), 0)
        down = lax.broadcasted_iota(jnp.int32, (slots, seqs), 0).astype(F32)
        across = lax.broadcasted_iota(jnp.int32, (seqs, slots), 1).astype(F32)
        base = jnp.zeros((experts, 1), F32)
        sent = jnp.zeros((slots, seqs), F32)
        for c in copies:
            c.wait()
        for k in range(top):
            row = ids[k : k + 1, :]
            mine = (number == row).astype(F32)
            before = dot(mine.astype(BF16), earlier) + base
            slot = jnp.sum(before * mine, axis=0, keepdims=True)
            base = base + jnp.sum(mine, axis=1, keepdims=True)
            part = jnp.floor((slot + 0.5) * (1 / half))
            place = part * (experts * half) + row.astype(F32) * half + (slot - part * half)
            sent = sent + (down == place).astype(F32)
            column = jnp.sum(jnp.where(one == other, place, 0.0), axis=1, keepdims=True)
            hits[k * seqs : (k + 1) * seqs, :] = (across == column).astype(F32).astype(BF16)
            column = jnp.sum(
                jnp.where(one == other, weight[k : k + 1, :], 0.0), axis=1, keepdims=True
            )
            wcol[k] = jnp.broadcast_to(column, wcol.shape[1:])
        named[...] = sent.astype(BF16)

    return pick_kernel


def mixer(t0, t2, t3, mix_row, b0, b1, g0, g1, out0, out1, rows0, rows1, state_out, keep, give):
    me = tp_index()
    seqs, quarter = t0.shape
    channels = rows0.shape[1]
    base = 2 * seqs + 8 + 2 * channels
    t1 = jnp.concatenate([rows1[i : i + seqs, :] for i in range(base, rows1.shape[0], seqs)], axis=1)
    pieces = [t0[...].astype(F32), t1, t2[...].astype(F32), t3[...].astype(F32)]
    squares = sum(jnp.sum(p * p, axis=1, keepdims=True) for p in pieces)
    scale = lax.rsqrt(squares / (len(pieces) * quarter) + EPS)
    sums = [0.0] * 4
    for k, p in enumerate(pieces):
        at = span(me ^ k, quarter)
        normed = (p * scale * mix_row[:, at]).astype(BF16)
        sums = [v + dot(normed, w[at, :]) for v, w in zip(sums, (b0, g0, b1, g1))]
    kept = given = 0.0
    own, beside = span(me, quarter), span(me ^ 3, quarter)
    for i, (rows, w_out) in enumerate(((rows0, out0), (rows1, out1))):
        branch, gate_in = (v.astype(BF16).astype(F32) for v in sums[2 * i : 2 * i + 2])
        conv_out = rows[:seqs, :] + branch * rows[2 * seqs : 2 * seqs + 1, :]
        heads = conv_out.astype(BF16)
        maps = 2 * seqs + 8
        recur = jax.nn.sigmoid(dot(heads, rows[maps : maps + channels, :].astype(BF16)))
        inject = jax.nn.sigmoid(dot(heads, rows[maps + channels : maps + 2 * channels, :].astype(BF16)))
        log_decay = recur * rows[2 * seqs + 1 : 2 * seqs + 2, :]
        y = -2.0 * log_decay
        series = y * (1.0 - y * (1 / 2) * (1.0 - y * (1 / 3) * (1.0 - y * (1 / 4) * (1.0 - y * (1 / 5)))))
        left = jnp.where(y < 0.1, series, 1.0 - jnp.exp(-y))
        out = jnp.exp(log_decay) * rows[seqs : 2 * seqs, :] + jnp.sqrt(left) * inject * conv_out
        if i == 0:
            state_out[...] = out
        lru_out = (out * jax.nn.gelu(gate_in)).astype(BF16)
        kept = kept + dot(lru_out, w_out[:, own])
        given = given + dot(lru_out, w_out[:, beside])
    keep[...] = kept
    give[...] = given.astype(BF16)


def send_rows(tokens, keep, other, named, resid, sent):
    mix_out = (keep[...] + other[...].astype(F32)).astype(BF16).astype(F32)
    rows = (tokens[...].astype(F32) + mix_out).astype(BF16)
    resid[...] = rows
    slots = named.shape[0]
    buffer = dot(named[...], rows).astype(BF16)
    for a in range(0, sent.shape[0], slots):
        sent[a : a + slots, :] = buffer


def experts_of(got, ffn_row, g0, u0, d0, g1, u1, d1, out, rows):
    count, quarter = rows.shape[0], got.shape[1]
    squares = 0.0
    for a in range(0, got.shape[0], count):
        v = got[a : a + count, :].astype(F32)
        squares = squares + jnp.sum(v * v, axis=1, keepdims=True)
    scale = lax.rsqrt(squares / rows.shape[1] + EPS)
    for t in range(got.shape[0] // count):
        at = slice(t * quarter, (t + 1) * quarter)
        v = got[t * count : (t + 1) * count, :].astype(F32)
        rows[:, at] = (v * scale * ffn_row[:, at]).astype(BF16)
    term = 0.0
    for g, u, d in ((g0, u0, d0), (g1, u1, d1)):
        hidden = (jax.nn.silu(dot(rows[...], g[0])) * dot(rows[...], u[0])).astype(BF16)
        term = term + dot(hidden, d[0])
    for t in range(got.shape[0] // count):
        out[t * count : (t + 1) * count, :] = term[:, t * quarter : (t + 1) * quarter].astype(BF16)


def combine(resid, back, hits, wcol, mixed):
    top, seqs, width = wcol.shape
    slots = hits.shape[1]
    picked = sum(dot(hits[...], back[a : a + slots, :]) for a in range(0, back.shape[0], slots))
    for i in range(0, resid.shape[1], width):
        total = resid[:, i : i + width].astype(F32)
        for k in range(top):
            total = total + picked[k * seqs : (k + 1) * seqs, i : i + width] * wcol[k]
        mixed[:, i : i + width] = total.astype(BF16)


def step(
    tokens,
    conv_state,
    lru_state,
    mix_gain,
    ffn_gain,
    w_branch,
    w_gate,
    conv_taps,
    w_recur,
    w_inject,
    lru_lambda,
    w_out,
    expert_gate,
    expert_up,
    expert_down,
    route_ids,
    route_weight,
):
    seqs, quarter = tokens.shape
    top = route_ids.shape[1]
    channels = lru_state.shape[1]
    tp = ("xa", "xb")
    na = lax.axis_size("xa")
    n_tp = na * lax.axis_size("xb")
    features = n_tp * quarter
    experts = lax.axis_size("ep") * expert_gate.shape[0]
    nb = lax.axis_size("xb")
    capacity = max(2, 2 * seqs * top // experts)
    half = -(-capacity // nb)
    slots = nb * experts * half
    ring = ("xa", "xb", "ep")

    def swapped(x, k):
        return lax.ppermute(x, tp, [(i, i ^ k) for i in range(n_tp)])

    others = [swapped(tokens, k) for k in range(2, n_tp)]

    def beside(x):
        return lax.ppermute(x, "xb", SWAP)

    b_1, g_1, out_1 = (beside(w) for w in (w_branch, w_gate, w_out))
    mixing = (
        conv_state.transpose(1, 0, 2),
        conv_taps,
        w_recur,
        w_inject,
        lru_lambda,
        lru_state,
        tokens,
    )
    rows_0, here = call(
        pack,
        [
            ((2 * seqs + 8 + 2 * channels + seqs * (quarter // channels), channels), F32),
            (tokens.shape, BF16),
        ],
        *mixing,
        far=len(mixing),
        scratch=[pltpu.VMEM(a.shape, a.dtype) for a in mixing[:5]]
        + [pltpu.SemaphoreType.DMA((len(mixing),))],
        flops=10**5,
    )
    rows_1 = beside(rows_0)
    large = (w_branch, w_gate, w_out)
    mix_row, ffn_row, b_0, g_0, out_0 = call(
        prepare,
        [((1, features), F32)] * 2 + [(a.shape, a.dtype) for a in large],
        mix_gain,
        ffn_gain,
        *large,
        rows_0,
        far=2 + len(large),
        scratch=[pltpu.VMEM(a.shape, a.dtype) for a in (mix_gain, ffn_gain)]
        + [pltpu.SemaphoreType.DMA((2 + len(large),))],
        flops=10**6,
    )
    state_out, keep, give = call(
        mixer,
        [((seqs, channels), F32), ((seqs, quarter), F32), ((seqs, quarter), BF16)],
        here,
        *others,
        mix_row,
        b_0,
        b_1,
        g_0,
        g_1,
        out_0,
        out_1,
        rows_0,
        rows_1,
        flops=10**8,
        final=(0,),
    )
    routes = (route_ids.T, route_weight.T)
    named, hits, wcol = call(
        pick(experts, half),
        [((slots, seqs), BF16), ((top * seqs, slots), BF16), ((top, seqs, 128), F32)],
        *routes,
        keep,
        far=2,
        scratch=[pltpu.VMEM(a.shape, a.dtype) for a in routes] + [pltpu.SemaphoreType.DMA((2,))],
        flops=10**6,
    )
    resid, sent = call(
        send_rows,
        [((seqs, quarter), BF16), ((na * slots, quarter), BF16)],
        here,
        keep,
        swapped(give, 3),
        named,
        flops=10**7,
    )
    partners = []
    for w in (expert_gate, expert_up, expert_down):
        partners.append(lax.ppermute(w, "xb", SWAP))
    arrived = lax.all_to_all(sent, ring, split_axis=0, concat_axis=0, tiled=True)
    (term,) = call(
        experts_of,
        [((na * slots, quarter), BF16)],
        arrived,
        ffn_row,
        expert_gate,
        expert_up,
        expert_down,
        *partners,
        scratch=[pltpu.VMEM((slots // nb, features), BF16)],
        flops=10**9,
        limit=8 << 20,
    )
    back = lax.all_to_all(term, ring, split_axis=0, concat_axis=0, tiled=True)
    (mixed,) = call(combine, [((seqs, quarter), BF16)], resid, back, hits, wcol, final=(0,))
    return (mixed, state_out)


def solution(mesh):
    n_ep, n_tp = mesh.shape["ep"], mesh.shape["tp"]
    finer = Mesh(np.asarray(mesh.devices).reshape(n_ep, n_tp // 2, 2), ("ep", "xa", "xb"))
    tp = ("xa", "xb")
    placed = (
        P("ep", tp),
        P("ep", None, tp),
        P("ep", tp),
        P(),
        P(),
        P(None, tp),
        P(None, tp),
        P(None, tp),
        P(tp, None, None),
        P(tp, None, None),
        P(tp),
        P(tp, None),
        P("ep", None, tp),
        P("ep", None, tp),
        P("ep", tp, None),
        P("ep", None),
        P("ep", None),
    )
    return jax.shard_map(step, mesh=finer, in_specs=placed, out_specs=(P("ep", tp), P("ep", tp)), check_vma=False)
```

```python
import jax
import jax.numpy as jnp
import numpy as np
from jax import lax
from jax.experimental import pallas as pl
from jax.experimental.pallas import tpu as pltpu
from jax.sharding import Mesh, PartitionSpec as P

EPS = 1e-06
LRU_SCALE = 8.0
SWAP = ((0, 1), (1, 0))
F32, BF16 = jnp.float32, jnp.bfloat16


def call(kernel, outs, *args, scratch=(), flops=0, final=(), limit=4 << 20, far=0):
    away = tuple(pltpu.with_memory_space_constraint(a, pltpu.HBM) for a in args[:far])
    near = tuple(pltpu.with_memory_space_constraint(a, pltpu.VMEM) for a in args[far:])
    return pl.pallas_call(
        kernel,
        out_shape=[
            jax.ShapeDtypeStruct(s, d) if i in final else pltpu.VMEM(s, d)
            for i, (s, d) in enumerate(outs)
        ],
        in_specs=[pl.BlockSpec(memory_space=pltpu.HBM)] * far
        + [pl.BlockSpec(memory_space=pltpu.VMEM)] * len(near),
        out_specs=[
            pl.BlockSpec(memory_space=pl.ANY if i in final else pltpu.VMEM) for i in range(len(outs))
        ],
        scratch_shapes=list(scratch),
        compiler_params=pltpu.CompilerParams(vmem_limit_bytes=limit),
        cost_estimate=pl.CostEstimate(flops=flops, bytes_accessed=0, transcendentals=0),
    )(*away, *near)


def dot(a, b):
    return jnp.dot(a, b, preferred_element_type=F32)


def tp_index():
    return lax.axis_index("xa") * lax.axis_size("xb") + lax.axis_index("xb")


def span(i, size):
    return pl.ds(pl.multiple_of(i * size, size), size)


def pack(conv_h, taps_h, wr_h, wi_h, lam_h, state_h, tok_h, rows, tok, conv, taps, wr, wi, lam, sem):
    seqs, channels = state_h.shape
    held = (conv, taps, wr, wi, lam)
    targets = held + (rows.at[seqs : 2 * seqs, :], tok)
    sources = (conv_h, taps_h, wr_h, wi_h, lam_h, state_h, tok_h)
    copies = [
        pltpu.make_async_copy(h, v, sem.at[i]) for i, (h, v) in enumerate(zip(sources, targets))
    ]
    for c in copies:
        c.start()
    ends = 2 * seqs
    rows[ends:, :] = jnp.zeros((rows.shape[0] - ends, channels), F32)
    for c in copies[: len(held)]:
        c.wait()
    total = conv[0].astype(F32) * taps[0:1, :].astype(F32)
    for j in range(1, conv.shape[0]):
        total = total + conv[j].astype(F32) * taps[j : j + 1, :].astype(F32)
    rows[:seqs, :] = total
    rows[ends : ends + 1, :] = taps[conv.shape[0] :, :].astype(F32)
    rows[ends + 1 : ends + 2, :] = -LRU_SCALE * jnp.log1p(jnp.exp(-lam[...])).reshape(1, -1)
    heads, width = wr.shape[0], wr.shape[1]
    for i, w in enumerate((wr, wi)):
        base = ends + 8 + i * channels
        for h in range(heads):
            at = slice(h * width, (h + 1) * width)
            rows[base + h * width : base + (h + 1) * width, at] = w[h].astype(F32)
    for c in copies[len(held) :]:
        c.wait()
    base = ends + 8 + 2 * channels
    for i in range(tok.shape[1] // channels):
        at = slice(i * channels, (i + 1) * channels)
        rows[base + i * seqs : base + (i + 1) * seqs, :] = tok[:, at].astype(F32)


def prepare(mix_h, ffn_h, b_h, g_h, o_h, _, mix_row, ffn_row, b, g, o, mix_gain, ffn_gain, sem):
    pairs = ((mix_h, mix_gain), (ffn_h, ffn_gain), (b_h, b), (g_h, g), (o_h, o))
    copies = [pltpu.make_async_copy(h, v, sem.at[i]) for i, (h, v) in enumerate(pairs)]
    for c in copies:
        c.start()
    for c in copies[:2]:
        c.wait()
    mix_row[...] = mix_gain[...].astype(F32).reshape(mix_row.shape)
    ffn_row[...] = ffn_gain[...].astype(F32).reshape(ffn_row.shape)
    for c in copies[2:]:
        c.wait()


def pick(experts, half):
    def pick_kernel(ids_h, weight_h, _, named, hits, wcol, ids, weight, sem):
        copies = [
            pltpu.make_async_copy(h, v, sem.at[i])
            for i, (h, v) in enumerate(((ids_h, ids), (weight_h, weight)))
        ]
        for c in copies:
            c.start()
        top, seqs = ids.shape
        slots = named.shape[0]
        one, other = (lax.broadcasted_iota(jnp.int32, (seqs, seqs), i) for i in range(2))
        earlier = (one < other).astype(BF16)
        number = lax.broadcasted_iota(jnp.int32, (experts, seqs), 0)
        down = lax.broadcasted_iota(jnp.int32, (slots, seqs), 0).astype(F32)
        across = lax.broadcasted_iota(jnp.int32, (seqs, slots), 1).astype(F32)
        base = jnp.zeros((experts, 1), F32)
        sent = jnp.zeros((slots, seqs), F32)
        for c in copies:
            c.wait()
        for k in range(top):
            row = ids[k : k + 1, :]
            mine = (number == row).astype(F32)
            before = dot(mine.astype(BF16), earlier) + base
            slot = jnp.sum(before * mine, axis=0, keepdims=True)
            base = base + jnp.sum(mine, axis=1, keepdims=True)
            part = jnp.floor((slot + 0.5) * (1 / half))
            place = part * (experts * half) + row.astype(F32) * half + (slot - part * half)
            sent = sent + (down == place).astype(F32)
            column = jnp.sum(jnp.where(one == other, place, 0.0), axis=1, keepdims=True)
            hits[k * seqs : (k + 1) * seqs, :] = (across == column).astype(F32).astype(BF16)
            column = jnp.sum(
                jnp.where(one == other, weight[k : k + 1, :], 0.0), axis=1, keepdims=True
            )
            wcol[k] = jnp.broadcast_to(column, wcol.shape[1:])
        named[...] = sent.astype(BF16)

    return pick_kernel


def mixer(t0, t2, t3, mix_row, b0, b1, g0, g1, out0, out1, rows0, rows1, state_out, keep, give):
    me = tp_index()
    seqs, quarter = t0.shape
    channels = rows0.shape[1]
    base = 2 * seqs + 8 + 2 * channels
    t1 = jnp.concatenate([rows1[i : i + seqs, :] for i in range(base, rows1.shape[0], seqs)], axis=1)
    pieces = [t0[...].astype(F32), t1, t2[...].astype(F32), t3[...].astype(F32)]
    squares = sum(jnp.sum(p * p, axis=1, keepdims=True) for p in pieces)
    scale = lax.rsqrt(squares / (len(pieces) * quarter) + EPS)
    sums = [0.0] * 4
    for k, p in enumerate(pieces):
        at = span(me ^ k, quarter)
        normed = (p * scale * mix_row[:, at]).astype(BF16)
        sums = [v + dot(normed, w[at, :]) for v, w in zip(sums, (b0, g0, b1, g1))]
    kept = given = 0.0
    own, beside = span(me, quarter), span(me ^ 3, quarter)
    for i, (rows, w_out) in enumerate(((rows0, out0), (rows1, out1))):
        branch, gate_in = (v.astype(BF16).astype(F32) for v in sums[2 * i : 2 * i + 2])
        conv_out = rows[:seqs, :] + branch * rows[2 * seqs : 2 * seqs + 1, :]
        heads = conv_out.astype(BF16)
        maps = 2 * seqs + 8
        recur = jax.nn.sigmoid(dot(heads, rows[maps : maps + channels, :].astype(BF16)))
        inject = jax.nn.sigmoid(dot(heads, rows[maps + channels : maps + 2 * channels, :].astype(BF16)))
        log_decay = recur * rows[2 * seqs + 1 : 2 * seqs + 2, :]
        y = -2.0 * log_decay
        series = y * (1.0 - y * (1 / 2) * (1.0 - y * (1 / 3) * (1.0 - y * (1 / 4) * (1.0 - y * (1 / 5)))))
        left = jnp.where(y < 0.1, series, 1.0 - jnp.exp(-y))
        out = jnp.exp(log_decay) * rows[seqs : 2 * seqs, :] + jnp.sqrt(left) * inject * conv_out
        if i == 0:
            state_out[...] = out
        lru_out = (out * jax.nn.gelu(gate_in)).astype(BF16)
        kept = kept + dot(lru_out, w_out[:, own])
        given = given + dot(lru_out, w_out[:, beside])
    keep[...] = kept
    give[...] = given.astype(BF16)


def send_rows(tokens, keep, other, named, resid, sent):
    mix_out = (keep[...] + other[...].astype(F32)).astype(BF16).astype(F32)
    rows = (tokens[...].astype(F32) + mix_out).astype(BF16)
    resid[...] = rows
    slots = named.shape[0]
    buffer = dot(named[...], rows).astype(BF16)
    for a in range(0, sent.shape[0], slots):
        sent[a : a + slots, :] = buffer


def experts_of(got, ffn_row, g0, u0, d0, g1, u1, d1, out, rows):
    count, quarter = rows.shape[0], got.shape[1]
    squares = 0.0
    for t in range(got.shape[0] // count):
        at = slice(t * quarter, (t + 1) * quarter)
        v = got[t * count : (t + 1) * count, :].astype(F32)
        rows[:, at] = (v * ffn_row[:, at]).astype(BF16)
        squares = squares + jnp.sum(v * v, axis=1, keepdims=True)
    scale = lax.rsqrt(squares / rows.shape[1] + EPS)
    term = 0.0
    for g, u, d in ((g0, u0, d0), (g1, u1, d1)):
        first, second = dot(rows[...], g[0]) * scale, dot(rows[...], u[0]) * scale
        term = term + dot((jax.nn.silu(first) * second).astype(BF16), d[0])
    for t in range(got.shape[0] // count):
        out[t * count : (t + 1) * count, :] = term[:, t * quarter : (t + 1) * quarter].astype(BF16)


def combine(resid, back, hits, wcol, state, mixed_h, state_h, mixed, sem):
    leaving = [pltpu.make_async_copy(state, state_h, sem.at[0])]
    leaving[0].start()
    top, seqs, width = wcol.shape
    slots = hits.shape[1]
    for j, i in enumerate(range(0, resid.shape[1], width)):
        at = slice(i, i + width)
        picked = sum(dot(hits[...], back[a : a + slots, at]) for a in range(0, back.shape[0], slots))
        total = resid[:, at].astype(F32)
        for k in range(top):
            total = total + picked[k * seqs : (k + 1) * seqs, :] * wcol[k]
        mixed[:, at] = total.astype(BF16)
        leaving.append(pltpu.make_async_copy(mixed.at[:, at], mixed_h.at[:, at], sem.at[j + 1]))
        leaving[-1].start()
    for c in leaving:
        c.wait()


def step(
    tokens,
    conv_state,
    lru_state,
    mix_gain,
    ffn_gain,
    w_branch,
    w_gate,
    conv_taps,
    w_recur,
    w_inject,
    lru_lambda,
    w_out,
    expert_gate,
    expert_up,
    expert_down,
    route_ids,
    route_weight,
):
    seqs, quarter = tokens.shape
    top = route_ids.shape[1]
    channels = lru_state.shape[1]
    tp = ("xa", "xb")
    na = lax.axis_size("xa")
    n_tp = na * lax.axis_size("xb")
    features = n_tp * quarter
    experts = lax.axis_size("ep") * expert_gate.shape[0]
    nb = lax.axis_size("xb")
    capacity = max(2, 2 * seqs * top // experts)
    half = -(-capacity // nb)
    slots = nb * experts * half
    ring = ("xa", "xb", "ep")

    def swapped(x, k):
        return lax.ppermute(x, tp, [(i, i ^ k) for i in range(n_tp)])

    others = [swapped(tokens, k) for k in range(2, n_tp)]

    def beside(x):
        return lax.ppermute(x, "xb", SWAP)

    b_1, g_1, out_1 = (beside(w) for w in (w_branch, w_gate, w_out))
    mixing = (
        conv_state.transpose(1, 0, 2),
        conv_taps,
        w_recur,
        w_inject,
        lru_lambda,
        lru_state,
        tokens,
    )
    rows_0, here = call(
        pack,
        [
            ((2 * seqs + 8 + 2 * channels + seqs * (quarter // channels), channels), F32),
            (tokens.shape, BF16),
        ],
        *mixing,
        far=len(mixing),
        scratch=[pltpu.VMEM(a.shape, a.dtype) for a in mixing[:5]]
        + [pltpu.SemaphoreType.DMA((len(mixing),))],
        flops=10**5,
    )
    rows_1 = beside(rows_0)
    large = (w_branch, w_gate, w_out)
    mix_row, ffn_row, b_0, g_0, out_0 = call(
        prepare,
        [((1, features), F32)] * 2 + [(a.shape, a.dtype) for a in large],
        mix_gain,
        ffn_gain,
        *large,
        rows_0,
        far=2 + len(large),
        scratch=[pltpu.VMEM(a.shape, a.dtype) for a in (mix_gain, ffn_gain)]
        + [pltpu.SemaphoreType.DMA((2 + len(large),))],
        flops=10**6,
    )
    state, keep, give = call(
        mixer,
        [((seqs, channels), F32), ((seqs, quarter), F32), ((seqs, quarter), BF16)],
        here,
        *others,
        mix_row,
        b_0,
        b_1,
        g_0,
        g_1,
        out_0,
        out_1,
        rows_0,
        rows_1,
        flops=10**8,
    )
    routes = (route_ids.T, route_weight.T)
    named, hits, wcol = call(
        pick(experts, half),
        [((slots, seqs), BF16), ((top * seqs, slots), BF16), ((top, seqs, 128), F32)],
        *routes,
        keep,
        far=2,
        scratch=[pltpu.VMEM(a.shape, a.dtype) for a in routes] + [pltpu.SemaphoreType.DMA((2,))],
        flops=10**6,
    )
    resid, sent = call(
        send_rows,
        [((seqs, quarter), BF16), ((na * slots, quarter), BF16)],
        here,
        keep,
        swapped(give, 3),
        named,
        flops=10**7,
    )
    partners = []
    for w in (expert_gate, expert_up, expert_down):
        partners.append(lax.ppermute(w, "xb", SWAP))
    arrived = lax.all_to_all(sent, ring, split_axis=0, concat_axis=0, tiled=True)
    (term,) = call(
        experts_of,
        [((na * slots, quarter), BF16)],
        arrived,
        ffn_row,
        expert_gate,
        expert_up,
        expert_down,
        *partners,
        scratch=[pltpu.VMEM((slots // nb, features), BF16)],
        flops=10**9,
        limit=8 << 20,
    )
    back = lax.all_to_all(term, ring, split_axis=0, concat_axis=0, tiled=True)
    return call(
        combine,
        [((seqs, quarter), BF16), ((seqs, channels), F32)],
        resid,
        back,
        hits,
        wcol,
        state,
        final=(0, 1),
        scratch=[pltpu.VMEM((seqs, quarter), BF16), pltpu.SemaphoreType.DMA((1 + quarter // 128,))],
    )


def solution(mesh):
    n_ep, n_tp = mesh.shape["ep"], mesh.shape["tp"]
    finer = Mesh(np.asarray(mesh.devices).reshape(n_ep, n_tp // 2, 2), ("ep", "xa", "xb"))
    tp = ("xa", "xb")
    placed = (
        P("ep", tp),
        P("ep", None, tp),
        P("ep", tp),
        P(),
        P(),
        P(None, tp),
        P(None, tp),
        P(None, tp),
        P(tp, None, None),
        P(tp, None, None),
        P(tp),
        P(tp, None),
        P("ep", None, tp),
        P("ep", None, tp),
        P("ep", tp, None),
        P("ep", None),
        P("ep", None),
    )
    return jax.shard_map(step, mesh=finer, in_specs=placed, out_specs=(P("ep", tp), P("ep", tp)), check_vma=False)
```

```python
import jax
import jax.numpy as jnp
import numpy as np
from jax import lax
from jax.experimental import pallas as pl
from jax.experimental.pallas import tpu as pltpu
from jax.sharding import Mesh, PartitionSpec as P

EPS = 1e-06
LRU_SCALE = 8.0
SWAP = ((0, 1), (1, 0))
F32, BF16 = jnp.float32, jnp.bfloat16


def call(kernel, outs, *args, scratch=(), flops=0, final=(), limit=4 << 20, far=0):
    away = tuple(pltpu.with_memory_space_constraint(a, pltpu.HBM) for a in args[:far])
    near = tuple(pltpu.with_memory_space_constraint(a, pltpu.VMEM) for a in args[far:])
    return pl.pallas_call(
        kernel,
        out_shape=[
            jax.ShapeDtypeStruct(s, d) if i in final else pltpu.VMEM(s, d)
            for i, (s, d) in enumerate(outs)
        ],
        in_specs=[pl.BlockSpec(memory_space=pltpu.HBM)] * far
        + [pl.BlockSpec(memory_space=pltpu.VMEM)] * len(near),
        out_specs=[
            pl.BlockSpec(memory_space=pl.ANY if i in final else pltpu.VMEM) for i in range(len(outs))
        ],
        scratch_shapes=list(scratch),
        compiler_params=pltpu.CompilerParams(vmem_limit_bytes=limit),
        cost_estimate=pl.CostEstimate(flops=flops, bytes_accessed=0, transcendentals=0),
    )(*away, *near)


def dot(a, b):
    return jnp.dot(a, b, preferred_element_type=F32)


def tp_index():
    return lax.axis_index("xa") * lax.axis_size("xb") + lax.axis_index("xb")


def span(i, size):
    return pl.ds(pl.multiple_of(i * size, size), size)


def pack(conv_h, taps_h, wr_h, wi_h, lam_h, state_h, tok_h, rows, tok, conv, taps, wr, wi, lam, sem):
    seqs, channels = state_h.shape
    held = (conv, taps, wr, wi, lam)
    targets = held + (rows.at[seqs : 2 * seqs, :], tok)
    sources = (conv_h, taps_h, wr_h, wi_h, lam_h, state_h, tok_h)
    copies = [
        pltpu.make_async_copy(h, v, sem.at[i]) for i, (h, v) in enumerate(zip(sources, targets))
    ]
    for c in copies:
        c.start()
    ends = 2 * seqs
    rows[ends:, :] = jnp.zeros((rows.shape[0] - ends, channels), F32)
    for c in copies[: len(held)]:
        c.wait()
    total = conv[0].astype(F32) * taps[0:1, :].astype(F32)
    for j in range(1, conv.shape[0]):
        total = total + conv[j].astype(F32) * taps[j : j + 1, :].astype(F32)
    rows[:seqs, :] = total
    rows[ends : ends + 1, :] = taps[conv.shape[0] :, :].astype(F32)
    rows[ends + 1 : ends + 2, :] = -LRU_SCALE * jnp.log1p(jnp.exp(-lam[...])).reshape(1, -1)
    heads, width = wr.shape[0], wr.shape[1]
    for i, w in enumerate((wr, wi)):
        base = ends + 8 + i * channels
        for h in range(heads):
            at = slice(h * width, (h + 1) * width)
            rows[base + h * width : base + (h + 1) * width, at] = w[h].astype(F32)
    for c in copies[len(held) :]:
        c.wait()
    base = ends + 8 + 2 * channels
    for i in range(tok.shape[1] // channels):
        at = slice(i * channels, (i + 1) * channels)
        rows[base + i * seqs : base + (i + 1) * seqs, :] = tok[:, at].astype(F32)


def prepare(mix_h, ffn_h, b_h, g_h, o_h, _, mix_row, ffn_row, b, g, o, mix_gain, ffn_gain, sem):
    pairs = ((mix_h, mix_gain), (ffn_h, ffn_gain), (b_h, b), (g_h, g), (o_h, o))
    copies = [pltpu.make_async_copy(h, v, sem.at[i]) for i, (h, v) in enumerate(pairs)]
    for c in copies:
        c.start()
    for c in copies[:2]:
        c.wait()
    mix_row[...] = mix_gain[...].astype(F32).reshape(mix_row.shape)
    ffn_row[...] = ffn_gain[...].astype(F32).reshape(ffn_row.shape)
    for c in copies[2:]:
        c.wait()


def pick(experts, capacity):
    def pick_kernel(ids_h, weight_h, _, named, hits, wcol, ids, weight, sem):
        copies = [
            pltpu.make_async_copy(h, v, sem.at[i])
            for i, (h, v) in enumerate(((ids_h, ids), (weight_h, weight)))
        ]
        for c in copies:
            c.start()
        top, seqs = ids.shape
        slots = named.shape[0]
        one, other = (lax.broadcasted_iota(jnp.int32, (seqs, seqs), i) for i in range(2))
        earlier = (one < other).astype(BF16)
        number = lax.broadcasted_iota(jnp.int32, (experts, seqs), 0)
        down = lax.broadcasted_iota(jnp.int32, (slots, seqs), 0).astype(F32)
        across = lax.broadcasted_iota(jnp.int32, (seqs, slots), 1).astype(F32)
        base = jnp.zeros((experts, 1), F32)
        sent = jnp.zeros((slots, seqs), F32)
        for c in copies:
            c.wait()
        for k in range(top):
            row = ids[k : k + 1, :]
            mine = (number == row).astype(F32)
            before = dot(mine.astype(BF16), earlier) + base
            slot = jnp.sum(before * mine, axis=0, keepdims=True)
            base = base + jnp.sum(mine, axis=1, keepdims=True)
            place = row.astype(F32) * capacity + slot
            sent = sent + (down == place).astype(F32)
            column = jnp.sum(jnp.where(one == other, place, 0.0), axis=1, keepdims=True)
            hits[k * seqs : (k + 1) * seqs, :] = (across == column).astype(F32).astype(BF16)
            column = jnp.sum(
                jnp.where(one == other, weight[k : k + 1, :], 0.0), axis=1, keepdims=True
            )
            wcol[k] = jnp.broadcast_to(column, wcol.shape[1:])
        named[...] = sent.astype(BF16)

    return pick_kernel


def mixer(t0, t2, t3, mix_row, b0, b1, g0, g1, out0, out1, rows0, rows1, state_out, keep, give):
    me = tp_index()
    seqs, quarter = t0.shape
    channels = rows0.shape[1]
    base = 2 * seqs + 8 + 2 * channels
    t1 = jnp.concatenate([rows1[i : i + seqs, :] for i in range(base, rows1.shape[0], seqs)], axis=1)
    pieces = [t0[...].astype(F32), t1, t2[...].astype(F32), t3[...].astype(F32)]
    squares = sum(jnp.sum(p * p, axis=1, keepdims=True) for p in pieces)
    scale = lax.rsqrt(squares / (len(pieces) * quarter) + EPS)
    sums = [0.0] * 4
    for k, p in enumerate(pieces):
        at = span(me ^ k, quarter)
        normed = (p * scale * mix_row[:, at]).astype(BF16)
        sums = [v + dot(normed, w[at, :]) for v, w in zip(sums, (b0, g0, b1, g1))]
    kept = given = 0.0
    own, beside = span(me, quarter), span(me ^ 3, quarter)
    for i, (rows, w_out) in enumerate(((rows0, out0), (rows1, out1))):
        branch, gate_in = (v.astype(BF16).astype(F32) for v in sums[2 * i : 2 * i + 2])
        conv_out = rows[:seqs, :] + branch * rows[2 * seqs : 2 * seqs + 1, :]
        heads = conv_out.astype(BF16)
        maps = 2 * seqs + 8
        recur = jax.nn.sigmoid(dot(heads, rows[maps : maps + channels, :].astype(BF16)))
        inject = jax.nn.sigmoid(dot(heads, rows[maps + channels : maps + 2 * channels, :].astype(BF16)))
        log_decay = recur * rows[2 * seqs + 1 : 2 * seqs + 2, :]
        y = -2.0 * log_decay
        series = y * (1.0 - y * (1 / 2) * (1.0 - y * (1 / 3) * (1.0 - y * (1 / 4) * (1.0 - y * (1 / 5)))))
        left = jnp.where(y < 0.1, series, 1.0 - jnp.exp(-y))
        out = jnp.exp(log_decay) * rows[seqs : 2 * seqs, :] + jnp.sqrt(left) * inject * conv_out
        if i == 0:
            state_out[...] = out
        lru_out = (out * jax.nn.gelu(gate_in)).astype(BF16)
        kept = kept + dot(lru_out, w_out[:, own])
        given = given + dot(lru_out, w_out[:, beside])
    keep[...] = kept
    give[...] = given.astype(BF16)


def send_rows(tokens, keep, other, named, resid, sent):
    mix_out = (keep[...] + other[...].astype(F32)).astype(BF16).astype(F32)
    rows = (tokens[...].astype(F32) + mix_out).astype(BF16)
    resid[...] = rows
    slots = named.shape[0]
    buffer = dot(named[...], rows).astype(BF16)
    for a in range(0, sent.shape[0], slots):
        sent[a : a + slots, :] = buffer


def experts_of(got, ffn_row, g0, u0, d0, g1, u1, d1, out, rows):
    na, sources, both, quarter = got.shape
    nb = rows.shape[1] // (na * quarter)
    half = both // nb
    blocks = [(x, slice(c * half, (c + 1) * half)) for x in range(na) for c in range(nb)]
    squares = 0.0
    for t, (x, part) in enumerate(blocks):
        at = slice(t * quarter, (t + 1) * quarter)
        v = got[x, :, part, :].reshape(sources * half, quarter).astype(F32)
        rows[:, at] = (v * ffn_row[:, at]).astype(BF16)
        squares = squares + jnp.sum(v * v, axis=1, keepdims=True)
    scale = lax.rsqrt(squares / rows.shape[1] + EPS)
    hidden = []
    for g, u in ((g0, u0), (g1, u1)):
        first, second = dot(rows[...], g[0]) * scale, dot(rows[...], u[0]) * scale
        hidden.append((jax.nn.silu(first) * second).astype(BF16))
    for t, (x, part) in enumerate(blocks):
        at = slice(t * quarter, (t + 1) * quarter)
        term = dot(hidden[0], d0[0, :, at]) + dot(hidden[1], d1[0, :, at])
        out[x, :, part, :] = term.astype(BF16).reshape(sources, half, quarter)


def combine(resid, back, hits, wcol, state, mixed_h, state_h, mixed, sem):
    leaving = [pltpu.make_async_copy(state, state_h, sem.at[0])]
    leaving[0].start()
    top, seqs, width = wcol.shape
    slots = hits.shape[1]
    for j, i in enumerate(range(0, resid.shape[1], width)):
        at = slice(i, i + width)
        picked = sum(dot(hits[...], back[a : a + slots, at]) for a in range(0, back.shape[0], slots))
        total = resid[:, at].astype(F32)
        for k in range(top):
            total = total + picked[k * seqs : (k + 1) * seqs, :] * wcol[k]
        mixed[:, at] = total.astype(BF16)
        leaving.append(pltpu.make_async_copy(mixed.at[:, at], mixed_h.at[:, at], sem.at[j + 1]))
        leaving[-1].start()
    for c in leaving:
        c.wait()


def step(
    tokens,
    conv_state,
    lru_state,
    mix_gain,
    ffn_gain,
    w_branch,
    w_gate,
    conv_taps,
    w_recur,
    w_inject,
    lru_lambda,
    w_out,
    expert_gate,
    expert_up,
    expert_down,
    route_ids,
    route_weight,
):
    seqs, quarter = tokens.shape
    top = route_ids.shape[1]
    channels = lru_state.shape[1]
    tp = ("xa", "xb")
    na = lax.axis_size("xa")
    n_tp = na * lax.axis_size("xb")
    features = n_tp * quarter
    experts = lax.axis_size("ep") * expert_gate.shape[0]
    nb = lax.axis_size("xb")
    capacity = max(2, 2 * seqs * top // experts)
    half = -(-capacity // nb)
    slots = nb * experts * half
    ring = ("xa", "ep", "xb")

    def swapped(x, k):
        return lax.ppermute(x, tp, [(i, i ^ k) for i in range(n_tp)])

    others = [swapped(tokens, k) for k in range(2, n_tp)]

    def beside(x):
        return lax.ppermute(x, "xb", SWAP)

    b_1, g_1, out_1 = (beside(w) for w in (w_branch, w_gate, w_out))
    mixing = (
        conv_state.transpose(1, 0, 2),
        conv_taps,
        w_recur,
        w_inject,
        lru_lambda,
        lru_state,
        tokens,
    )
    rows_0, here = call(
        pack,
        [
            ((2 * seqs + 8 + 2 * channels + seqs * (quarter // channels), channels), F32),
            (tokens.shape, BF16),
        ],
        *mixing,
        far=len(mixing),
        scratch=[pltpu.VMEM(a.shape, a.dtype) for a in mixing[:5]]
        + [pltpu.SemaphoreType.DMA((len(mixing),))],
        flops=10**5,
    )
    rows_1 = beside(rows_0)
    large = (w_branch, w_gate, w_out)
    mix_row, ffn_row, b_0, g_0, out_0 = call(
        prepare,
        [((1, features), F32)] * 2 + [(a.shape, a.dtype) for a in large],
        mix_gain,
        ffn_gain,
        *large,
        rows_0,
        far=2 + len(large),
        scratch=[pltpu.VMEM(a.shape, a.dtype) for a in (mix_gain, ffn_gain)]
        + [pltpu.SemaphoreType.DMA((2 + len(large),))],
        flops=10**6,
    )
    state, keep, give = call(
        mixer,
        [((seqs, channels), F32), ((seqs, quarter), F32), ((seqs, quarter), BF16)],
        here,
        *others,
        mix_row,
        b_0,
        b_1,
        g_0,
        g_1,
        out_0,
        out_1,
        rows_0,
        rows_1,
        flops=5*10**9,
    )
    routes = (route_ids.T, route_weight.T)
    named, hits, wcol = call(
        pick(experts, nb * half),
        [((slots, seqs), BF16), ((top * seqs, slots), BF16), ((top, seqs, 128), F32)],
        *routes,
        keep,
        far=2,
        scratch=[pltpu.VMEM(a.shape, a.dtype) for a in routes] + [pltpu.SemaphoreType.DMA((2,))],
        flops=10**6,
    )
    resid, sent = call(
        send_rows,
        [((seqs, quarter), BF16), ((na * slots, quarter), BF16)],
        here,
        keep,
        swapped(give, 3),
        named,
        flops=10**7,
    )
    partners = []
    for w in (expert_gate, expert_up, expert_down):
        partners.append(lax.ppermute(w, "xb", SWAP))
    blocks = (na, experts, nb * half, quarter)
    arrived = lax.all_to_all(sent, ring, split_axis=0, concat_axis=0, tiled=True)
    (term,) = call(
        experts_of,
        [(blocks, BF16)],
        arrived.reshape(blocks),
        ffn_row,
        expert_gate,
        expert_up,
        expert_down,
        *partners,
        scratch=[pltpu.VMEM((slots // nb, features), BF16)],
        flops=10**9,
        limit=8 << 20,
    )
    back = lax.all_to_all(term.reshape(na * slots, quarter), ring, split_axis=0, concat_axis=0, tiled=True)
    return call(
        combine,
        [((seqs, quarter), BF16), ((seqs, channels), F32)],
        resid,
        back,
        hits,
        wcol,
        state,
        final=(0, 1),
        scratch=[pltpu.VMEM((seqs, quarter), BF16), pltpu.SemaphoreType.DMA((1 + quarter // 128,))],
    )


def solution(mesh):
    n_ep, n_tp = mesh.shape["ep"], mesh.shape["tp"]
    finer = Mesh(np.asarray(mesh.devices).reshape(n_ep, n_tp // 2, 2), ("ep", "xa", "xb"))
    tp = ("xa", "xb")
    placed = (
        P("ep", tp),
        P("ep", None, tp),
        P("ep", tp),
        P(),
        P(),
        P(None, tp),
        P(None, tp),
        P(None, tp),
        P(tp, None, None),
        P(tp, None, None),
        P(tp),
        P(tp, None),
        P("ep", None, tp),
        P("ep", None, tp),
        P("ep", tp, None),
        P("ep", None),
        P("ep", None),
    )
    return jax.shard_map(step, mesh=finer, in_specs=placed, out_specs=(P("ep", tp), P("ep", tp)), check_vma=False)
```

```python
import jax
import jax.numpy as jnp
import numpy as np
from jax import lax
from jax.experimental import pallas as pl
from jax.experimental.pallas import tpu as pltpu
from jax.sharding import Mesh, PartitionSpec as P

EPS = 1e-06
LRU_SCALE = 8.0
SWAP = ((0, 1), (1, 0))
F32, BF16 = jnp.float32, jnp.bfloat16


def call(kernel, outs, *args, scratch=(), flops=0, final=(), limit=4 << 20, far=0):
    away = tuple(pltpu.with_memory_space_constraint(a, pltpu.HBM) for a in args[:far])
    near = tuple(pltpu.with_memory_space_constraint(a, pltpu.VMEM) for a in args[far:])
    return pl.pallas_call(
        kernel,
        out_shape=[
            jax.ShapeDtypeStruct(s, d) if i in final else pltpu.VMEM(s, d)
            for i, (s, d) in enumerate(outs)
        ],
        in_specs=[pl.BlockSpec(memory_space=pltpu.HBM)] * far
        + [pl.BlockSpec(memory_space=pltpu.VMEM)] * len(near),
        out_specs=[
            pl.BlockSpec(memory_space=pl.ANY if i in final else pltpu.VMEM) for i in range(len(outs))
        ],
        scratch_shapes=list(scratch),
        compiler_params=pltpu.CompilerParams(vmem_limit_bytes=limit),
        cost_estimate=pl.CostEstimate(flops=flops, bytes_accessed=0, transcendentals=0),
    )(*away, *near)


def dot(a, b):
    return jnp.dot(a, b, preferred_element_type=F32)


def tp_index():
    return lax.axis_index("xa") * lax.axis_size("xb") + lax.axis_index("xb")


def span(i, size):
    return pl.ds(pl.multiple_of(i * size, size), size)


def pack(conv_h, taps_h, wr_h, wi_h, lam_h, state_h, tok_h, rows, tok, conv, taps, wr, wi, lam, sem):
    seqs, channels = state_h.shape
    held = (conv, taps, wr, wi, lam)
    targets = held + (rows.at[seqs : 2 * seqs, :], tok)
    sources = (conv_h, taps_h, wr_h, wi_h, lam_h, state_h, tok_h)
    copies = [
        pltpu.make_async_copy(h, v, sem.at[i]) for i, (h, v) in enumerate(zip(sources, targets))
    ]
    for c in copies:
        c.start()
    ends = 2 * seqs
    rows[ends : ends + 8, :] = jnp.zeros((8, channels), F32)
    for c in copies[: len(held)]:
        c.wait()
    total = conv[0].astype(F32) * taps[0:1, :].astype(F32)
    for j in range(1, conv.shape[0]):
        total = total + conv[j].astype(F32) * taps[j : j + 1, :].astype(F32)
    rows[:seqs, :] = total
    rows[ends : ends + 1, :] = taps[conv.shape[0] :, :].astype(F32)
    rows[ends + 1 : ends + 2, :] = -LRU_SCALE * jnp.log1p(jnp.exp(-lam[...])).reshape(1, -1)
    heads, width = wr.shape[0], wr.shape[1]
    for i, w in enumerate((wr, wi)):
        base = ends + 8 + i * width
        for h in range(heads):
            rows[base : base + width, h * width : (h + 1) * width] = w[h].astype(F32)
    for c in copies[len(held) :]:
        c.wait()
    base = ends + 8 + 2 * width
    for i in range(tok.shape[1] // channels):
        at = slice(i * channels, (i + 1) * channels)
        rows[base + i * seqs : base + (i + 1) * seqs, :] = tok[:, at].astype(F32)


def prepare(mix_h, ffn_h, b_h, g_h, o_h, _, mix_row, ffn_row, b, g, o, mix_gain, ffn_gain, sem):
    pairs = ((mix_h, mix_gain), (ffn_h, ffn_gain), (b_h, b), (g_h, g), (o_h, o))
    copies = [pltpu.make_async_copy(h, v, sem.at[i]) for i, (h, v) in enumerate(pairs)]
    for c in copies:
        c.start()
    for c in copies[:2]:
        c.wait()
    mix_row[...] = mix_gain[...].astype(F32).reshape(mix_row.shape)
    ffn_row[...] = ffn_gain[...].astype(F32).reshape(ffn_row.shape)
    for c in copies[2:]:
        c.wait()


def pick(experts, capacity):
    def pick_kernel(ids_h, weight_h, _, named, hits, wcol, ids, weight, sem):
        copies = [
            pltpu.make_async_copy(h, v, sem.at[i])
            for i, (h, v) in enumerate(((ids_h, ids), (weight_h, weight)))
        ]
        for c in copies:
            c.start()
        top, seqs = ids.shape
        slots = named.shape[0]
        one, other = (lax.broadcasted_iota(jnp.int32, (seqs, seqs), i) for i in range(2))
        earlier = (one < other).astype(BF16)
        number = lax.broadcasted_iota(jnp.int32, (experts, seqs), 0)
        down = lax.broadcasted_iota(jnp.int32, (slots, seqs), 0).astype(F32)
        across = lax.broadcasted_iota(jnp.int32, (seqs, slots), 1).astype(F32)
        base = jnp.zeros((experts, 1), F32)
        sent = jnp.zeros((slots, seqs), F32)
        for c in copies:
            c.wait()
        for k in range(top):
            row = ids[k : k + 1, :]
            mine = (number == row).astype(F32)
            before = dot(mine.astype(BF16), earlier) + base
            slot = jnp.sum(before * mine, axis=0, keepdims=True)
            base = base + jnp.sum(mine, axis=1, keepdims=True)
            place = row.astype(F32) * capacity + slot
            sent = sent + (down == place).astype(F32)
            column = jnp.sum(jnp.where(one == other, place, 0.0), axis=1, keepdims=True)
            hits[k * seqs : (k + 1) * seqs, :] = (across == column).astype(F32).astype(BF16)
            column = jnp.sum(
                jnp.where(one == other, weight[k : k + 1, :], 0.0), axis=1, keepdims=True
            )
            wcol[k] = jnp.broadcast_to(column, wcol.shape[1:])
        named[...] = sent.astype(BF16)

    return pick_kernel


def mixer(t0, t2, t3, mix_row, b0, b1, g0, g1, out0, out1, rows0, rows1, state_out, keep, give):
    me = tp_index()
    seqs, quarter = t0.shape
    channels = rows0.shape[1]
    base = rows0.shape[0] - seqs * (quarter // channels)
    width = (base - 2 * seqs - 8) // 2
    shape = (channels, channels)
    inside = (
        lax.broadcasted_iota(jnp.int32, shape, 0) // width
        == lax.broadcasted_iota(jnp.int32, shape, 1) // width
    )

    def spread(maps):
        return jnp.where(inside, jnp.concatenate([maps] * (channels // width), axis=0), 0.0).astype(BF16)

    t1 = jnp.concatenate([rows1[i : i + seqs, :] for i in range(base, rows1.shape[0], seqs)], axis=1)
    pieces = [t0[...].astype(F32), t1, t2[...].astype(F32), t3[...].astype(F32)]
    squares = sum(jnp.sum(p * p, axis=1, keepdims=True) for p in pieces)
    scale = lax.rsqrt(squares / (len(pieces) * quarter) + EPS)
    sums = [0.0] * 4
    for k, p in enumerate(pieces):
        at = span(me ^ k, quarter)
        normed = (p * scale * mix_row[:, at]).astype(BF16)
        sums = [v + dot(normed, w[at, :]) for v, w in zip(sums, (b0, g0, b1, g1))]
    kept = given = 0.0
    own, beside = span(me, quarter), span(me ^ 3, quarter)
    for i, (rows, w_out) in enumerate(((rows0, out0), (rows1, out1))):
        branch, gate_in = (v.astype(BF16).astype(F32) for v in sums[2 * i : 2 * i + 2])
        conv_out = rows[:seqs, :] + branch * rows[2 * seqs : 2 * seqs + 1, :]
        heads = conv_out.astype(BF16)
        maps = 2 * seqs + 8
        recur = jax.nn.sigmoid(dot(heads, spread(rows[maps : maps + width, :])))
        inject = jax.nn.sigmoid(dot(heads, spread(rows[maps + width : base, :])))
        log_decay = recur * rows[2 * seqs + 1 : 2 * seqs + 2, :]
        y = -2.0 * log_decay
        series = y * (1.0 - y * (1 / 2) * (1.0 - y * (1 / 3) * (1.0 - y * (1 / 4) * (1.0 - y * (1 / 5)))))
        left = jnp.where(y < 0.1, series, 1.0 - jnp.exp(-y))
        out = jnp.exp(log_decay) * rows[seqs : 2 * seqs, :] + jnp.sqrt(left) * inject * conv_out
        if i == 0:
            state_out[...] = out
        lru_out = (out * jax.nn.gelu(gate_in)).astype(BF16)
        kept = kept + dot(lru_out, w_out[:, own])
        given = given + dot(lru_out, w_out[:, beside])
    keep[...] = kept
    give[...] = given.astype(BF16)


def send_rows(tokens, keep, other, named, resid, sent):
    mix_out = (keep[...] + other[...].astype(F32)).astype(BF16).astype(F32)
    rows = (tokens[...].astype(F32) + mix_out).astype(BF16)
    resid[...] = rows
    slots = named.shape[0]
    buffer = dot(named[...], rows).astype(BF16)
    for a in range(0, sent.shape[0], slots):
        sent[a : a + slots, :] = buffer


def experts_of(got, ffn_row, g0, u0, d0, g1, u1, d1, out, rows):
    na, sources, both, quarter = got.shape
    nb = rows.shape[1] // (na * quarter)
    half = both // nb
    blocks = [(x, slice(c * half, (c + 1) * half)) for x in range(na) for c in range(nb)]
    squares = 0.0
    for t, (x, part) in enumerate(blocks):
        at = slice(t * quarter, (t + 1) * quarter)
        v = got[x, :, part, :].reshape(sources * half, quarter).astype(F32)
        rows[:, at] = (v * ffn_row[:, at]).astype(BF16)
        squares = squares + jnp.sum(v * v, axis=1, keepdims=True)
    scale = lax.rsqrt(squares / rows.shape[1] + EPS)
    hidden = []
    for g, u in ((g0, u0), (g1, u1)):
        first, second = dot(rows[...], g[0]) * scale, dot(rows[...], u[0]) * scale
        hidden.append((jax.nn.silu(first) * second).astype(BF16))
    for t, (x, part) in enumerate(blocks):
        at = slice(t * quarter, (t + 1) * quarter)
        term = dot(hidden[0], d0[0, :, at]) + dot(hidden[1], d1[0, :, at])
        out[x, :, part, :] = term.astype(BF16).reshape(sources, half, quarter)


def combine(resid, back, hits, wcol, state, mixed_h, state_h, mixed, sem):
    leaving = [pltpu.make_async_copy(state, state_h, sem.at[0])]
    leaving[0].start()
    top, seqs, width = wcol.shape
    slots = hits.shape[1]
    for j, i in enumerate(range(0, resid.shape[1], width)):
        at = slice(i, i + width)
        picked = sum(dot(hits[...], back[a : a + slots, at]) for a in range(0, back.shape[0], slots))
        total = resid[:, at].astype(F32)
        for k in range(top):
            total = total + picked[k * seqs : (k + 1) * seqs, :] * wcol[k]
        mixed[:, at] = total.astype(BF16)
        leaving.append(pltpu.make_async_copy(mixed.at[:, at], mixed_h.at[:, at], sem.at[j + 1]))
        leaving[-1].start()
    for c in leaving:
        c.wait()


def step(
    tokens,
    conv_state,
    lru_state,
    mix_gain,
    ffn_gain,
    w_branch,
    w_gate,
    conv_taps,
    w_recur,
    w_inject,
    lru_lambda,
    w_out,
    expert_gate,
    expert_up,
    expert_down,
    route_ids,
    route_weight,
):
    seqs, quarter = tokens.shape
    top = route_ids.shape[1]
    channels = lru_state.shape[1]
    tp = ("xa", "xb")
    na = lax.axis_size("xa")
    n_tp = na * lax.axis_size("xb")
    features = n_tp * quarter
    experts = lax.axis_size("ep") * expert_gate.shape[0]
    nb = lax.axis_size("xb")
    capacity = max(2, 2 * seqs * top // experts)
    half = -(-capacity // nb)
    slots = nb * experts * half
    ring = ("xa", "ep", "xb")

    def swapped(x, k):
        return lax.ppermute(x, tp, [(i, i ^ k) for i in range(n_tp)])

    others = [swapped(tokens, k) for k in range(2, n_tp)]

    def beside(x):
        return lax.ppermute(x, "xb", SWAP)

    b_1, g_1, out_1 = (beside(w) for w in (w_branch, w_gate, w_out))
    mixing = (
        conv_state.transpose(1, 0, 2),
        conv_taps,
        w_recur,
        w_inject,
        lru_lambda,
        lru_state,
        tokens,
    )
    rows_0, here = call(
        pack,
        [((2 * seqs + 8 + 2 * w_recur.shape[1] + seqs * (quarter // channels), channels), F32), (tokens.shape, BF16)],
        *mixing,
        far=len(mixing),
        scratch=[pltpu.VMEM(a.shape, a.dtype) for a in mixing[:5]]
        + [pltpu.SemaphoreType.DMA((len(mixing),))],
        flops=10**5,
    )
    rows_1 = beside(rows_0)
    large = (w_branch, w_gate, w_out)
    mix_row, ffn_row, b_0, g_0, out_0 = call(
        prepare,
        [((1, features), F32)] * 2 + [(a.shape, a.dtype) for a in large],
        mix_gain,
        ffn_gain,
        *large,
        rows_0,
        far=2 + len(large),
        scratch=[pltpu.VMEM(a.shape, a.dtype) for a in (mix_gain, ffn_gain)]
        + [pltpu.SemaphoreType.DMA((2 + len(large),))],
        flops=10**6,
    )
    state, keep, give = call(
        mixer,
        [((seqs, channels), F32), ((seqs, quarter), F32), ((seqs, quarter), BF16)],
        here,
        *others,
        mix_row,
        b_0,
        b_1,
        g_0,
        g_1,
        out_0,
        out_1,
        rows_0,
        rows_1,
        flops=5*10**9,
    )
    routes = (route_ids.T, route_weight.T)
    named, hits, wcol = call(
        pick(experts, nb * half),
        [((slots, seqs), BF16), ((top * seqs, slots), BF16), ((top, seqs, 128), F32)],
        *routes,
        keep,
        far=2,
        scratch=[pltpu.VMEM(a.shape, a.dtype) for a in routes] + [pltpu.SemaphoreType.DMA((2,))],
        flops=10**6,
    )
    resid, sent = call(
        send_rows,
        [((seqs, quarter), BF16), ((na * slots, quarter), BF16)],
        here,
        keep,
        swapped(give, 3),
        named,
        flops=10**7,
    )
    partners = []
    for w in (expert_gate, expert_up, expert_down):
        partners.append(lax.ppermute(w, "xb", SWAP))
    blocks = (na, experts, nb * half, quarter)
    arrived = lax.all_to_all(sent, ring, split_axis=0, concat_axis=0, tiled=True)
    (term,) = call(
        experts_of,
        [(blocks, BF16)],
        arrived.reshape(blocks),
        ffn_row,
        expert_gate,
        expert_up,
        expert_down,
        *partners,
        scratch=[pltpu.VMEM((slots // nb, features), BF16)],
        flops=10**9,
        limit=8 << 20,
    )
    back = lax.all_to_all(term.reshape(na * slots, quarter), ring, split_axis=0, concat_axis=0, tiled=True)
    return call(
        combine,
        [((seqs, quarter), BF16), ((seqs, channels), F32)],
        resid,
        back,
        hits,
        wcol,
        state,
        final=(0, 1),
        scratch=[pltpu.VMEM((seqs, quarter), BF16), pltpu.SemaphoreType.DMA((1 + quarter // 128,))],
    )


def solution(mesh):
    n_ep, n_tp = mesh.shape["ep"], mesh.shape["tp"]
    finer = Mesh(np.asarray(mesh.devices).reshape(n_ep, n_tp // 2, 2), ("ep", "xa", "xb"))
    tp = ("xa", "xb")
    placed = (
        P("ep", tp),
        P("ep", None, tp),
        P("ep", tp),
        P(),
        P(),
        P(None, tp),
        P(None, tp),
        P(None, tp),
        P(tp, None, None),
        P(tp, None, None),
        P(tp),
        P(tp, None),
        P("ep", None, tp),
        P("ep", None, tp),
        P("ep", tp, None),
        P("ep", None),
        P("ep", None),
    )
    return jax.shard_map(step, mesh=finer, in_specs=placed, out_specs=(P("ep", tp), P("ep", tp)), check_vma=False)
```

```python
import jax
import jax.numpy as jnp
import numpy as np
from jax import lax
from jax.experimental import pallas as pl
from jax.experimental.pallas import tpu as pltpu
from jax.sharding import Mesh, PartitionSpec as P

EPS = 1e-06
LRU_SCALE = 8.0
SWAP = ((0, 1), (1, 0))
F32, BF16 = jnp.float32, jnp.bfloat16


def call(kernel, outs, *args, scratch=(), flops=0, final=(), limit=4 << 20, far=0):
    away = tuple(pltpu.with_memory_space_constraint(a, pltpu.HBM) for a in args[:far])
    near = tuple(pltpu.with_memory_space_constraint(a, pltpu.VMEM) for a in args[far:])
    return pl.pallas_call(
        kernel,
        out_shape=[
            jax.ShapeDtypeStruct(s, d) if i in final else pltpu.VMEM(s, d)
            for i, (s, d) in enumerate(outs)
        ],
        in_specs=[pl.BlockSpec(memory_space=pltpu.HBM)] * far
        + [pl.BlockSpec(memory_space=pltpu.VMEM)] * len(near),
        out_specs=[
            pl.BlockSpec(memory_space=pl.ANY if i in final else pltpu.VMEM) for i in range(len(outs))
        ],
        scratch_shapes=list(scratch),
        compiler_params=pltpu.CompilerParams(vmem_limit_bytes=limit),
        cost_estimate=pl.CostEstimate(flops=flops, bytes_accessed=0, transcendentals=0),
    )(*away, *near)


def dot(a, b):
    return jnp.dot(a, b, preferred_element_type=F32)


def tp_index():
    return lax.axis_index("xa") * lax.axis_size("xb") + lax.axis_index("xb")


def span(i, size):
    return pl.ds(pl.multiple_of(i * size, size), size)


def pack(conv_h, taps_h, wr_h, wi_h, lam_h, state_h, tok_h, rows, tok, conv, taps, wr, wi, lam, sem):
    seqs, channels = state_h.shape
    held = (conv, taps, wr, wi, lam)
    targets = held + (rows.at[seqs : 2 * seqs, :], tok)
    sources = (conv_h, taps_h, wr_h, wi_h, lam_h, state_h, tok_h)
    copies = [
        pltpu.make_async_copy(h, v, sem.at[i]) for i, (h, v) in enumerate(zip(sources, targets))
    ]
    for c in copies:
        c.start()
    ends = 2 * seqs
    rows[ends : ends + 8, :] = jnp.zeros((8, channels), F32)
    for c in copies[: len(held)]:
        c.wait()
    total = conv[0].astype(F32) * taps[0:1, :].astype(F32)
    for j in range(1, conv.shape[0]):
        total = total + conv[j].astype(F32) * taps[j : j + 1, :].astype(F32)
    rows[:seqs, :] = total
    rows[ends : ends + 1, :] = taps[conv.shape[0] :, :].astype(F32)
    rows[ends + 1 : ends + 2, :] = -LRU_SCALE * jnp.log1p(jnp.exp(-lam[...])).reshape(1, -1)
    heads, width = wr.shape[0], wr.shape[1]
    for i, w in enumerate((wr, wi)):
        base = ends + 8 + i * width
        for h in range(heads):
            rows[base : base + width, h * width : (h + 1) * width] = w[h].astype(F32)
    for c in copies[len(held) :]:
        c.wait()
    base = ends + 8 + 2 * width
    for i in range(tok.shape[1] // channels):
        at = slice(i * channels, (i + 1) * channels)
        rows[base + i * seqs : base + (i + 1) * seqs, :] = tok[:, at].astype(F32)


def prepare(mix_h, ffn_h, b_h, g_h, o_h, _, mix_row, ffn_row, b, g, o, mix_gain, ffn_gain, sem):
    pairs = ((mix_h, mix_gain), (ffn_h, ffn_gain), (b_h, b), (g_h, g), (o_h, o))
    copies = [pltpu.make_async_copy(h, v, sem.at[i]) for i, (h, v) in enumerate(pairs)]
    for c in copies:
        c.start()
    for c in copies[:2]:
        c.wait()
    mix_row[...] = mix_gain[...].astype(F32).reshape(mix_row.shape)
    ffn_row[...] = ffn_gain[...].astype(F32).reshape(ffn_row.shape)
    for c in copies[2:]:
        c.wait()


def pick(experts, capacity):
    def pick_kernel(ids_h, weight_h, _, named, hits, wcol, ids, weight, sem):
        copies = [
            pltpu.make_async_copy(h, v, sem.at[i])
            for i, (h, v) in enumerate(((ids_h, ids), (weight_h, weight)))
        ]
        for c in copies:
            c.start()
        top, seqs = ids.shape
        slots = named.shape[0]
        one, other = (lax.broadcasted_iota(jnp.int32, (seqs, seqs), i) for i in range(2))
        earlier = (one < other).astype(BF16)
        number = lax.broadcasted_iota(jnp.int32, (experts, seqs), 0)
        down = lax.broadcasted_iota(jnp.int32, (slots, seqs), 0).astype(F32)
        across = lax.broadcasted_iota(jnp.int32, (seqs, slots), 1).astype(F32)
        base = jnp.zeros((experts, 1), F32)
        sent = jnp.zeros((slots, seqs), F32)
        for c in copies:
            c.wait()
        for k in range(top):
            row = ids[k : k + 1, :]
            mine = (number == row).astype(F32)
            before = dot(mine.astype(BF16), earlier) + base
            slot = jnp.sum(before * mine, axis=0, keepdims=True)
            base = base + jnp.sum(mine, axis=1, keepdims=True)
            place = row.astype(F32) * capacity + slot
            sent = sent + (down == place).astype(F32)
            column = jnp.sum(jnp.where(one == other, place, 0.0), axis=1, keepdims=True)
            hits[k * seqs : (k + 1) * seqs, :] = (across == column).astype(F32).astype(BF16)
            column = jnp.sum(
                jnp.where(one == other, weight[k : k + 1, :], 0.0), axis=1, keepdims=True
            )
            wcol[k] = jnp.broadcast_to(column, wcol.shape[1:])
        named[...] = sent.astype(BF16)

    return pick_kernel


def mixer(t0, t2, t3, mix_row, b0, b1, g0, g1, out0, out1, rows0, rows1, state_out, keep, give):
    me = tp_index()
    seqs, quarter = t0.shape
    channels = rows0.shape[1]
    base = rows0.shape[0] - seqs * (quarter // channels)
    width = (base - 2 * seqs - 8) // 2
    shape = (channels, channels)
    inside = (
        lax.broadcasted_iota(jnp.int32, shape, 0) // width
        == lax.broadcasted_iota(jnp.int32, shape, 1) // width
    )

    def spread(maps):
        return jnp.where(inside, jnp.concatenate([maps] * (channels // width), axis=0), 0.0).astype(BF16)

    t1 = jnp.concatenate([rows1[i : i + seqs, :] for i in range(base, rows1.shape[0], seqs)], axis=1)
    pieces = [t0[...].astype(F32), t1, t2[...].astype(F32), t3[...].astype(F32)]
    squares = sum(jnp.sum(p * p, axis=1, keepdims=True) for p in pieces)
    scale = lax.rsqrt(squares / (len(pieces) * quarter) + EPS)
    sums = [0.0] * 4
    for k, p in enumerate(pieces):
        at = span(me ^ k, quarter)
        normed = (p * scale * mix_row[:, at]).astype(BF16)
        sums = [v + dot(normed, w[at, :]) for v, w in zip(sums, (b0, g0, b1, g1))]
    kept = given = 0.0
    own, beside = span(me, quarter), span(me ^ 3, quarter)
    for i, (rows, w_out) in enumerate(((rows0, out0), (rows1, out1))):
        branch, gate_in = (v.astype(BF16).astype(F32) for v in sums[2 * i : 2 * i + 2])
        conv_out = rows[:seqs, :] + branch * rows[2 * seqs : 2 * seqs + 1, :]
        heads = conv_out.astype(BF16)
        maps = 2 * seqs + 8
        recur = jax.nn.sigmoid(dot(heads, spread(rows[maps : maps + width, :])))
        inject = jax.nn.sigmoid(dot(heads, spread(rows[maps + width : base, :])))
        log_decay = recur * rows[2 * seqs + 1 : 2 * seqs + 2, :]
        y = -2.0 * log_decay
        series = y * (1.0 - y * (1 / 2) * (1.0 - y * (1 / 3) * (1.0 - y * (1 / 4) * (1.0 - y * (1 / 5)))))
        left = jnp.where(y < 0.1, series, 1.0 - jnp.exp(-y))
        out = jnp.exp(log_decay) * rows[seqs : 2 * seqs, :] + jnp.sqrt(left) * inject * conv_out
        if i == 0:
            state_out[...] = out
        lru_out = (out * jax.nn.gelu(gate_in)).astype(BF16)
        kept = kept + dot(lru_out, w_out[:, own])
        given = given + dot(lru_out, w_out[:, beside])
    keep[...] = kept
    give[...] = given.astype(BF16)


def send_rows(tokens, keep, other, named, resid, sent):
    mix_out = (keep[...] + other[...].astype(F32)).astype(BF16).astype(F32)
    rows = (tokens[...].astype(F32) + mix_out).astype(BF16)
    resid[...] = rows
    slots = named.shape[0]
    buffer = dot(named[...], rows).astype(BF16)
    for a in range(0, sent.shape[0], slots):
        sent[a : a + slots, :] = buffer


def experts_of(got, ffn_row, g0, u0, d0, g1, u1, d1, state, out, state_h, rows, sem):
    leaving = pltpu.make_async_copy(state, state_h, sem)
    leaving.start()
    na, sources, both, quarter = got.shape
    nb = rows.shape[1] // (na * quarter)
    half = both // nb
    blocks = [(x, slice(c * half, (c + 1) * half)) for x in range(na) for c in range(nb)]
    squares = 0.0
    for t, (x, part) in enumerate(blocks):
        at = slice(t * quarter, (t + 1) * quarter)
        v = got[x, :, part, :].reshape(sources * half, quarter).astype(F32)
        rows[:, at] = (v * ffn_row[:, at]).astype(BF16)
        squares = squares + jnp.sum(v * v, axis=1, keepdims=True)
    scale = lax.rsqrt(squares / rows.shape[1] + EPS)
    hidden = []
    for g, u in ((g0, u0), (g1, u1)):
        first, second = dot(rows[...], g[0]) * scale, dot(rows[...], u[0]) * scale
        hidden.append((jax.nn.silu(first) * second).astype(BF16))
    for t, (x, part) in enumerate(blocks):
        at = slice(t * quarter, (t + 1) * quarter)
        term = dot(hidden[0], d0[0, :, at]) + dot(hidden[1], d1[0, :, at])
        out[x, :, part, :] = term.astype(BF16).reshape(sources, half, quarter)
    leaving.wait()


def combine(resid, back, hits, wcol, mixed_h, mixed, sem):
    leaving = []
    top, seqs, width = wcol.shape
    slots = hits.shape[1]
    for j, i in enumerate(range(0, resid.shape[1], width)):
        at = slice(i, i + width)
        picked = sum(dot(hits[...], back[a : a + slots, at]) for a in range(0, back.shape[0], slots))
        total = resid[:, at].astype(F32)
        for k in range(top):
            total = total + picked[k * seqs : (k + 1) * seqs, :] * wcol[k]
        mixed[:, at] = total.astype(BF16)
        leaving.append(pltpu.make_async_copy(mixed.at[:, at], mixed_h.at[:, at], sem.at[j]))
        leaving[-1].start()
    for c in leaving:
        c.wait()


def step(
    tokens,
    conv_state,
    lru_state,
    mix_gain,
    ffn_gain,
    w_branch,
    w_gate,
    conv_taps,
    w_recur,
    w_inject,
    lru_lambda,
    w_out,
    expert_gate,
    expert_up,
    expert_down,
    route_ids,
    route_weight,
):
    seqs, quarter = tokens.shape
    top = route_ids.shape[1]
    channels = lru_state.shape[1]
    tp = ("xa", "xb")
    na = lax.axis_size("xa")
    n_tp = na * lax.axis_size("xb")
    features = n_tp * quarter
    experts = lax.axis_size("ep") * expert_gate.shape[0]
    nb = lax.axis_size("xb")
    capacity = max(2, 2 * seqs * top // experts)
    half = -(-capacity // nb)
    slots = nb * experts * half
    ring = ("xa", "ep", "xb")

    def swapped(x, k):
        return lax.ppermute(x, tp, [(i, i ^ k) for i in range(n_tp)])

    others = [swapped(tokens, k) for k in range(2, n_tp)]

    def beside(x):
        return lax.ppermute(x, "xb", SWAP)

    b_1, g_1, out_1 = (beside(w) for w in (w_branch, w_gate, w_out))
    mixing = (
        conv_state.transpose(1, 0, 2),
        conv_taps,
        w_recur,
        w_inject,
        lru_lambda,
        lru_state,
        tokens,
    )
    rows_0, here = call(
        pack,
        [((2 * seqs + 8 + 2 * w_recur.shape[1] + seqs * (quarter // channels), channels), F32), (tokens.shape, BF16)],
        *mixing,
        far=len(mixing),
        scratch=[pltpu.VMEM(a.shape, a.dtype) for a in mixing[:5]]
        + [pltpu.SemaphoreType.DMA((len(mixing),))],
        flops=10**5,
    )
    rows_1 = beside(rows_0)
    large = (w_branch, w_gate, w_out)
    mix_row, ffn_row, b_0, g_0, out_0 = call(
        prepare,
        [((1, features), F32)] * 2 + [(a.shape, a.dtype) for a in large],
        mix_gain,
        ffn_gain,
        *large,
        rows_0,
        far=2 + len(large),
        scratch=[pltpu.VMEM(a.shape, a.dtype) for a in (mix_gain, ffn_gain)]
        + [pltpu.SemaphoreType.DMA((2 + len(large),))],
        flops=10**6,
    )
    state, keep, give = call(
        mixer,
        [((seqs, channels), F32), ((seqs, quarter), F32), ((seqs, quarter), BF16)],
        here,
        *others,
        mix_row,
        b_0,
        b_1,
        g_0,
        g_1,
        out_0,
        out_1,
        rows_0,
        rows_1,
        flops=5*10**9,
    )
    routes = (route_ids.T, route_weight.T)
    named, hits, wcol = call(
        pick(experts, nb * half),
        [((slots, seqs), BF16), ((top * seqs, slots), BF16), ((top, seqs, 128), F32)],
        *routes,
        keep,
        far=2,
        scratch=[pltpu.VMEM(a.shape, a.dtype) for a in routes] + [pltpu.SemaphoreType.DMA((2,))],
        flops=10**6,
    )
    resid, sent = call(
        send_rows,
        [((seqs, quarter), BF16), ((na * slots, quarter), BF16)],
        here,
        keep,
        swapped(give, 3),
        named,
        flops=10**7,
    )
    partners = []
    for w in (expert_gate, expert_up, expert_down):
        partners.append(lax.ppermute(w, "xb", SWAP))
    blocks = (na, experts, nb * half, quarter)
    arrived = lax.all_to_all(sent, ring, split_axis=0, concat_axis=0, tiled=True)
    term, state_out = call(
        experts_of,
        [(blocks, BF16), ((seqs, channels), F32)],
        arrived.reshape(blocks),
        ffn_row,
        expert_gate,
        expert_up,
        expert_down,
        *partners,
        state,
        final=(1,),
        scratch=[pltpu.VMEM((slots // nb, features), BF16), pltpu.SemaphoreType.DMA],
        flops=10**9,
        limit=8 << 20,
    )
    back = lax.all_to_all(term.reshape(na * slots, quarter), ring, split_axis=0, concat_axis=0, tiled=True)
    (mixed,) = call(
        combine,
        [((seqs, quarter), BF16)],
        resid,
        back,
        hits,
        wcol,
        final=(0,),
        scratch=[pltpu.VMEM((seqs, quarter), BF16), pltpu.SemaphoreType.DMA((quarter // 128,))],
    )
    return (mixed, state_out)


def solution(mesh):
    n_ep, n_tp = mesh.shape["ep"], mesh.shape["tp"]
    finer = Mesh(np.asarray(mesh.devices).reshape(n_ep, n_tp // 2, 2), ("ep", "xa", "xb"))
    tp = ("xa", "xb")
    placed = (
        P("ep", tp),
        P("ep", None, tp),
        P("ep", tp),
        P(),
        P(),
        P(None, tp),
        P(None, tp),
        P(None, tp),
        P(tp, None, None),
        P(tp, None, None),
        P(tp),
        P(tp, None),
        P("ep", None, tp),
        P("ep", None, tp),
        P("ep", tp, None),
        P("ep", None),
        P("ep", None),
    )
    return jax.shard_map(step, mesh=finer, in_specs=placed, out_specs=(P("ep", tp), P("ep", tp)), check_vma=False)
```
